512 devices in a mesh: ep: 32 (over z, core), tp: 16 (over y, x).
Axes of the slice: x: 4, y: 4, z: 16, core: 2. Of those that a mesh axis runs over, the one named last changes fastest.
Arguments:
- query_rows: bfloat16 [16384, 2048], P('ep', 'tp'), may hold values from -6 to 6
- key_rows: bfloat16 [16384, 2048], P('ep', 'tp'), may hold values from -6 to 6
- value_rows: bfloat16 [16384, 4096], P('ep', 'tp'), may hold values from -6 to 6
- in_gate: float32 [16, 16384], P('tp', 'ep'), may hold values from -120 to 120
- forget_gate: float32 [16, 16384], P('tp', 'ep'), may hold values from -2 to 20
- out_gate: bfloat16 [16384, 4096], P('ep', 'tp'), may hold values from -6 to 6
- head_gain: float32 [4096], P('tp'), may hold values from 0.1 to 1.9
- mix_weight: bfloat16 [4096, 4096], P(None, 'tp'), may hold values from -0.09375 to 0.09375
- expert_input: bfloat16 [8192, 4096], P('ep', 'tp'), may hold values from -30 to 30
- routes: int32 [8192, 2], P('ep'), may hold values from 0 to 31, all different within a row; in each aligned block of 256 rows (0 to 255, 256 to 511, ...) at most 32 rows name the same one
- route_weight: float32 [8192, 2], P('ep'), may hold values from 0.25 to 1.25
- gate_weight: bfloat16 [32, 1024, 4096], P('ep', 'tp'), may hold values from -0.09375 to 0.09375
- up_weight: bfloat16 [32, 1024, 4096], P('ep', 'tp'), may hold values from -0.09375 to 0.09375
- down_weight: bfloat16 [32, 1024, 4096], P('ep', None, 'tp'), may hold values from -0.1875 to 0.1875
Outputs:
- mixer_out: bfloat16 [16384, 4096], P('ep', 'tp')
- expert_out: bfloat16 [8192, 4096], P('ep', 'tp')
The draws below stay inside these ranges and needn't reach their ends.
Inputs may be any that keep to these rules, and one draw needn't show every extreme that they name: `routes`: each row names 2 different experts. In the rows of one device no expert is named by more than 32 rows, and in the rows of some device an expert is named by exactly 32 rows.
All inputs are finite; a program needn't handle non-finite values.
Results may differ from the reference program's by a relative error of at most 0.0057.
Values may be sent and summed in bfloat16 or wider, within the bound.
A program may use at most 128 MiB of HBM per device.

```python
import math
import jax
import jax.numpy as jnp
import numpy as np
from jax import lax

D = 4096
HEADS = 16
QK = 128
FF = 1024
TOP = 2
BLOCK = 64
ROWS_A = 512
ROWS_B = 256
TOKENS_A = 16384
TOKENS_B = 8192
EXPERTS = 32
CAP = 32
N_EP = 32


def draw_in_gate(key, part):
    base = jnp.clip(jax.random.normal(jax.random.fold_in(key, 11), (HEADS, TOKENS_A), jnp.float32), -4.0, 4.0)
    return base


def draw_forget_gate(key, part):
    slow_share = 0.5
    slow_heads = jax.random.bernoulli(jax.random.fold_in(key, 21), slow_share, (HEADS, 1))
    level = jnp.where(slow_heads, math.log(TOKENS_A) + 0.5, 3.5)
    span_total = TOKENS_A // ROWS_A
    drift = jax.random.uniform(jax.random.fold_in(key, 22), (HEADS, span_total), jnp.float32, -1.0, 1.0)
    noise = 0.7 * jnp.clip(jax.random.normal(jax.random.fold_in(key, 23), (HEADS, TOKENS_A), jnp.float32), -4.0, 4.0)
    return level + jnp.repeat(drift, ROWS_A, axis=1) + noise


def draw_expert_input(key, part):
    row_scale = jnp.exp(jax.random.uniform(jax.random.fold_in(key, 31), (TOKENS_B, 1), jnp.float32, -0.7, 0.7))
    base = jnp.clip(jax.random.normal(jax.random.fold_in(key, 34), (TOKENS_B, D), jnp.float32), -4.0, 4.0)
    return (base * row_scale).astype(jnp.bfloat16)


def steps_of(rng, extent, split, low, high):
    loudness, own = 1.0, jax.random.fold_in(rng, 6)
    for axis_at, shards_of in split:
        steps = jnp.exp(jax.random.uniform(jax.random.fold_in(own, axis_at), (shards_of,), jnp.float32, low / len(split), high / len(split)))
        loudness = loudness * jnp.repeat(steps, extent[axis_at] // shards_of).reshape([-1 if axis == axis_at else 1 for axis in range(len(extent))])
    return loudness


def deal_out(key, own, number, rows, count, top, bound, slope):
    order = jax.random.permutation(key, count)
    packed, usual = load_shares(count, rows * top, bound, slope, True), load_shares(count, rows * top, bound, slope, False)
    places = jnp.arange(count)

    def named(tallies, offset_by):
        used = int((tallies > 0).sum())
        fixed = max(1, used // 4)
        shifted = fixed + (places - fixed + offset_by * (used - fixed)) % max(1, count - fixed)
        return jnp.zeros((count,), jnp.int32).at[order[jnp.where(places < fixed, places, shifted)]].set(jnp.asarray(tallies, jnp.int32))

    tallies = jnp.where(number % 4 == 0, named(packed, number // 4), named(usual, number - number // 4 - 1))
    mixed = jax.random.permutation(jax.random.fold_in(own, 3), count)
    donor, taker = mixed[0:count // 2 * 2:2], mixed[1:count // 2 * 2:2]
    room = jnp.minimum(tallies[donor] - 1, bound - tallies[taker]) // 2
    room = jnp.where((donor == order[0]) | (taker == order[0]) | (tallies[taker] == 0), 0, jnp.maximum(room, 0))
    shifted = jax.random.randint(jax.random.fold_in(own, 4), (count // 2,), 0, 1 << 20) % (room + 1)
    tallies = tallies.at[donor].add(-shifted).at[taker].add(shifted)
    labels = jnp.searchsorted(jnp.cumsum(tallies), jnp.arange(rows * top), side="right").astype(jnp.int32)
    listing = labels.reshape(top, rows).T
    listing = listing[jax.random.permutation(jax.random.fold_in(own, 1), rows)]
    offset_by = jax.random.randint(jax.random.fold_in(own, 2), (rows, 1), 0, top)
    return jnp.take_along_axis(listing, (jnp.arange(top)[None, :] + offset_by) % top, axis=1)


def load_shares(amount, total, bound, lean, full):
    weights = [(1 << 20) // math.isqrt(grade ** lean) + 1 for grade in range(1, amount + 1)]
    largest = bound if full else min(bound, max(-(-total // amount), total * weights[0] // sum(weights)))
    least = 1 if total - largest >= amount - 1 else 0
    given, rest = [largest] + [least] * (amount - 1), total - largest - least * (amount - 1)
    while rest > 0:
        free = [i for i in range(1, amount) if given[i] < largest] or [i for i in range(1, amount) if given[i] < bound]
        mass, remaining = sum([weights[i] for i in free]), rest
        for i in free:
            extra = min(bound - given[i], max(1, remaining * weights[i] // mass), rest)
            given[i] = given[i] + extra
            rest = rest - extra
    return np.array(given)


def centred(key, dims, scale, bound, cuts=(), kind=jnp.bfloat16):
    level = steps_of(key, dims, cuts, -0.22, 0.18) if cuts else 1.0
    entries = jax.random.normal(key, dims, jnp.float32) * scale * level
    return jnp.minimum(jnp.maximum(entries, -bound), bound).astype(kind)


def setup_inputs(seed: int = 0) -> dict:
    key_of = jax.random.split(jax.random.key(seed), 15)
    query_rows = centred(key_of[0], (TOKENS_A, HEADS * QK), 1.0, 6.0, ((0, 32), (1, 16)))
    key_rows = centred(key_of[1], (TOKENS_A, HEADS * QK), 1.0, 6.0, ((0, 32), (1, 16)))
    value_rows = centred(key_of[2], (TOKENS_A, D), 1.0, 6.0, ((0, 32), (1, 16)))
    in_gate = draw_in_gate(jax.random.fold_in(key_of[14], 71), 0)
    forget_gate = draw_forget_gate(jax.random.fold_in(key_of[14], 71), 0)
    out_gate = centred(key_of[5], (TOKENS_A, D), 1.0, 6.0, ((0, 32), (1, 16)))
    head_gain = jnp.clip(1.0 + 0.18 * jax.random.normal(key_of[6], (D,), jnp.float32), 0.1, 1.9)
    mix_weight = centred(key_of[7], (D, D), D ** -0.5, 0.09375, ((1, 16),))
    expert_input = draw_expert_input(jax.random.fold_in(key_of[14], 71), 0)
    routes_keys = jax.random.split(jax.random.fold_in(key_of[9], 1), TOKENS_B // ROWS_B)
    routes_turns = jax.random.permutation(jax.random.fold_in(key_of[9], 3), TOKENS_B // ROWS_B)
    routes = jax.vmap(lambda own, number: deal_out(jax.random.fold_in(key_of[9], 2), own, number, ROWS_B, EXPERTS, TOP, CAP, 1))(routes_keys, routes_turns).reshape((TOKENS_B, TOP))
    route_weight = jnp.clip(0.25 + 1.0 * jax.random.uniform(key_of[10], (TOKENS_B, TOP), jnp.float32) ** steps_of(key_of[10], (TOKENS_B, TOP), ((0, 32),), -0.2, 0.2), 0.25, 1.25)
    gate_weight = centred(key_of[11], (EXPERTS, FF, D), D ** -0.5, 0.09375, ((0, 32), (1, 16)))
    up_weight = centred(key_of[12], (EXPERTS, FF, D), D ** -0.5, 0.09375, ((0, 32), (1, 16)))
    down_weight = centred(key_of[13], (EXPERTS, FF, D), FF ** -0.5, 0.1875, ((0, 32), (2, 16)))
    return dict(query_rows=query_rows, key_rows=key_rows, value_rows=value_rows, in_gate=in_gate, forget_gate=forget_gate, out_gate=out_gate, head_gain=head_gain, mix_weight=mix_weight, expert_input=expert_input, routes=routes, route_weight=route_weight, gate_weight=gate_weight, up_weight=up_weight, down_weight=down_weight)


EPSILON = 1e-06
LOG_FLOOR = -1e+30
HIGHEST_PRECISION = lax.Precision.HIGHEST

def combine(first_part, second_part):
    decay_first, max_first, memory_first, normal_first = first_part
    decay_second, max_second, memory_second, normal_second = second_part
    running_max = jnp.maximum(decay_second + max_first, max_second)
    keep_first = jnp.exp(decay_second + max_first - running_max)
    keep_second = jnp.exp(max_second - running_max)
    memory = keep_first[..., None, None] * memory_first + keep_second[..., None, None] * memory_second
    normalizer = keep_first[..., None] * normal_first + keep_second[..., None] * normal_second
    return (decay_first + decay_second, running_max, memory, normalizer)

def identity_state(head_count, key_width, value_width):
    return (jnp.zeros((head_count,), jnp.float32), jnp.full((head_count,), LOG_FLOOR, jnp.float32), jnp.zeros((head_count, key_width, value_width), jnp.float32), jnp.zeros((head_count, key_width), jnp.float32))

def halfprod(form, left, right):
    return jnp.einsum(form, left.astype(jnp.float32), right.astype(jnp.float32), precision=HIGHEST_PRECISION)

def prepare(query_heads, key_heads, value_heads, in_gate, forget_gate):
    head_count, length, key_width = query_heads.shape
    block_count = length // BLOCK
    query_blocks = query_heads.reshape(head_count, block_count, BLOCK, key_width)
    key_blocks = key_heads.reshape(head_count, block_count, BLOCK, key_width)
    value_blocks = value_heads.reshape(head_count, block_count, BLOCK, value_heads.shape[-1])
    log_input = in_gate.reshape(head_count, block_count, BLOCK)
    cumulative = jnp.cumsum(jax.nn.log_sigmoid(forget_gate).reshape(head_count, block_count, BLOCK), axis=-1)
    block_decay = cumulative[..., -1]
    weight_log = block_decay[..., None] - cumulative + log_input
    block_max = lax.optimization_barrier(jnp.max(weight_log, axis=-1))
    weighted = key_blocks.astype(jnp.float32) * jnp.exp(weight_log - block_max[..., None])[..., None]
    normalizer = lax.optimization_barrier(jnp.sum(weighted, axis=2))
    memory = halfprod('hcsk,hcsv->hckv', weighted.astype(jnp.bfloat16), value_blocks)
    return ((query_blocks, key_blocks, value_blocks, log_input, cumulative), (block_decay, block_max, memory, normalizer))

def prefix(summary, initial):
    leading = jax.tree.map(lambda tensor: jnp.moveaxis(tensor, 1, 0), summary)

    def advance(running, current):
        return (combine(running, current), running)
    final_state, before = lax.scan(advance, initial, leading)
    return (final_state, jax.tree.map(lambda tensor: jnp.moveaxis(tensor, 0, 1), before))

def block_outputs(blocked, before):
    query_blocks, key_blocks, value_blocks, log_input, cumulative = blocked
    prior_max, prior_memory, prior_normal = (before[1], before[2], before[3])
    block_len = cumulative.shape[-1]
    scale = query_blocks.shape[-1] ** (-0.5)
    causal = jnp.tril(jnp.ones((block_len, block_len), dtype=bool))
    log_decay = jnp.where(causal, cumulative[..., :, None] - cumulative[..., None, :] + log_input[..., None, :], -jnp.inf)
    log_inter = cumulative + prior_max[..., None]
    top_value = jnp.maximum(log_inter, lax.optimization_barrier(jnp.max(log_decay, axis=-1)))
    scores = halfprod('hctk,hcsk->hcts', query_blocks, key_blocks) * scale * jnp.exp(log_decay - top_value[..., None])
    carried = jnp.exp(log_inter - top_value) * scale
    query_wide = query_blocks.astype(jnp.float32)
    numerator = carried[..., None] * jnp.einsum('hctk,hckv->hctv', query_wide, prior_memory, precision=HIGHEST_PRECISION) + halfprod('hcts,hcsv->hctv', scores.astype(jnp.bfloat16), value_blocks)
    denominator = carried * jnp.einsum('hctk,hck->hct', query_wide, prior_normal, precision=HIGHEST_PRECISION) + lax.optimization_barrier(jnp.sum(scores, axis=-1))
    return numerator / jnp.maximum(jnp.abs(denominator), jnp.exp(-top_value))[..., None]

def finish(head_values, out_gate, head_gain):
    head_count, block_count, block_len, value_width = head_values.shape
    per_head = jnp.transpose(head_values, (1, 2, 0, 3)).reshape(block_count * block_len, head_count, value_width)
    per_head = per_head * lax.rsqrt(lax.optimization_barrier(jnp.mean(per_head * per_head, axis=-1, keepdims=True)) + EPSILON)
    per_head = per_head.reshape(block_count * block_len, head_count * value_width) * head_gain
    per_head = per_head * jax.nn.sigmoid(out_gate.astype(jnp.float32))
    return per_head.astype(jnp.bfloat16)

def reference(query_rows, key_rows, value_rows, in_gate, forget_gate, out_gate, head_gain, mix_weight, expert_input, routes, route_weight, gate_weight, up_weight, down_weight):
    length = query_rows.shape[0]
    head_count = in_gate.shape[0]
    key_width = query_rows.shape[1] // head_count
    value_width = value_rows.shape[1] // head_count
    query_heads = query_rows.reshape(length, head_count, key_width).transpose(1, 0, 2)
    key_heads = key_rows.reshape(length, head_count, key_width).transpose(1, 0, 2)
    value_heads = value_rows.reshape(length, head_count, value_width).transpose(1, 0, 2)

    def one_head(current):
        query_one, key_one, value_one, input_one, forget_one = current
        blocked, summary = prepare(query_one[None], key_one[None], value_one[None], input_one[None], forget_one[None])
        final_state, before = prefix(summary, identity_state(1, key_width, value_width))
        return block_outputs(blocked, before)[0]
    head_values = lax.map(one_head, (query_heads, key_heads, value_heads, in_gate, forget_gate))
    mixed_heads = finish(head_values, out_gate, head_gain)
    mixer_out = jnp.dot(mixed_heads, mix_weight, preferred_element_type=jnp.float32).astype(jnp.bfloat16)
    squares = lax.optimization_barrier(jnp.sum(jnp.square(expert_input.astype(jnp.float32)), axis=-1))
    inverse_rms = lax.rsqrt(squares / D + EPSILON)
    slot_total = N_EP * CAP

    def one_expert(running, expert):
        matched = routes == expert
        picked = jnp.any(matched, axis=1)
        row_index = jnp.nonzero(picked, size=slot_total, fill_value=0)[0].astype(jnp.int32)
        count = jnp.sum(picked.astype(jnp.int32))
        is_valid = (jnp.arange(slot_total, dtype=jnp.int32) < count).astype(jnp.float32)
        weight = lax.optimization_barrier(jnp.sum(jnp.where(matched, route_weight, 0.0), axis=1))
        chosen = expert_input[row_index]
        row_scale = inverse_rms[row_index][:, None]
        gate_value = jnp.dot(chosen, gate_weight[expert].T, preferred_element_type=jnp.float32) * row_scale
        up_value = jnp.dot(chosen, up_weight[expert].T, preferred_element_type=jnp.float32) * row_scale
        hidden = (jax.nn.silu(gate_value) * up_value).astype(jnp.bfloat16)
        expert_rows = jnp.dot(hidden, down_weight[expert], preferred_element_type=jnp.float32).astype(jnp.bfloat16)
        term = expert_rows.astype(jnp.float32) * (weight[row_index] * is_valid)[:, None]
        return (running.at[row_index].add(term), None)
    total, _ = lax.scan(one_expert, jnp.zeros((TOKENS_B, D), jnp.float32), jnp.arange(EXPERTS, dtype=jnp.int32))
    return (mixer_out, total.astype(jnp.bfloat16))
```

```python
import functools

import jax
import jax.numpy as jnp
from jax import lax
from jax.experimental import pallas as pl
from jax.experimental.pallas import tpu as pltpu
from jax.sharding import PartitionSpec as P

MESH = pl.DeviceIdType.MESH
BF, F32 = jnp.bfloat16, jnp.float32
D = 4096
EPS = 1e-6
FLOOR = -1e30
NEG = -3e38
SCALE = 128**-0.5
HOPS = [8, 7, 9, 6, 10, 5, 11, 4, 12, 3, 13, 2, 14, 1, 15, 0]
NT = (((1,), (1,)), ((), ()))
TN = (((0,), (0,)), ((), ()))


def mm(a, b):
    return jnp.dot(a, b, preferred_element_type=F32)


def dg(a, b, dims):
    return lax.dot_general(a, b, dims, preferred_element_type=F32)


def kernel(
    q_ref, k_ref, v_ref, ig_ref, fg_ref, og_ref, gain_ref, mixw_hbm, x_ref, routes_ref, rw_ref,
    gate_hbm, up_hbm, down_hbm,
    out_a, out_b,
    mixw, downn, downt, wt, xs, xa, gsend, grecv, hid, rows, ret, mixed,
    p1s, p1r, auxr, p2s, p2r, seen, sel0, sel1, num_ref, col_ref,
    loc_sem, own_sem, w_send, w_recv, p_send, p_recv, d_send, d_recv,
    xg_send, xg_recv, g_send, g_recv, ag_send, ag_recv, r_send, r_recv,
):
    e, t = lax.axis_index("ep"), lax.axis_index("tp")
    z, c = e // 2, e % 2
    y, x = t // 4, t % 4

    def along(axis, d):
        return (e, y * 4 + (x + d) % 4) if axis == "x" else (e, ((y + d) % 4) * 4 + x)

    def send(src, dst, ss, rs, dev):
        copy = pltpu.make_async_remote_copy(
            src_ref=src, dst_ref=dst, send_sem=ss, recv_sem=rs, device_id=dev, device_id_type=MESH
        )
        copy.start()
        sends.append(copy)
        return copy

    def bytes_of(ref, sem):
        pltpu.make_async_copy(ref, ref, sem).wait()

    sends = []
    live = {}

    barrier = pltpu.get_barrier_semaphore()

    def hello(k, _):
        pl.semaphore_signal(barrier, inc=1, device_id=((e + k) % 32, t), device_id_type=MESH)
        return 0

    lax.fori_loop(1, 32, hello, 0)
    for axis in "xy":
        for d in (1, 2, 3):
            pl.semaphore_signal(barrier, inc=1, device_id=along(axis, d), device_id_type=MESH)

    own_g = pltpu.make_async_copy(
        gate_hbm.at[:, pl.ds(pl.multiple_of(y * 1024, 1024), 1024)], wt.at[y, pl.ds(0, 64)], own_sem.at[0]
    )
    own_u = pltpu.make_async_copy(
        up_hbm.at[:, pl.ds(pl.multiple_of(y * 1024, 1024), 1024)], wt.at[y, pl.ds(64, 64)], own_sem.at[1]
    )
    own_g.start()
    own_u.start()
    load_mix = pltpu.make_async_copy(mixw_hbm, mixw, loc_sem.at[0])
    load_down = pltpu.make_async_copy(down_hbm, downn, loc_sem.at[1])
    load_mix.start()
    load_down.start()
    turned = []
    for b in range(16):
        copy = pltpu.make_async_copy(
            down_hbm.at[pl.ds(64 * ((b % 4) * 4 + b // 4), 64)], downt.at[pl.ds(64 * b, 64)], loc_sem.at[2 + b]
        )
        copy.start()
        turned.append(copy)

    f = fg_ref[...]
    log_f = jnp.minimum(f, 0.0) - jnp.log1p(jnp.exp(-jnp.abs(f)))
    si = lax.broadcasted_iota(jnp.int32, (128, 512), 1)
    ri = lax.broadcasted_iota(jnp.int32, (128, 512), 0)
    c_row = jnp.zeros((1, 512), F32)
    for b in range(4):
        ti = ri + 128 * b
        col_ref[128 * b : 128 * b + 128, 0:1] = jnp.sum(
            jnp.where(si <= ti, log_f, 0.0), axis=1, keepdims=True
        )
        f_col = jnp.sum(jnp.where(si == ti, log_f, 0.0), axis=1, keepdims=True)
        c_row = c_row + jnp.sum(jnp.where(ti <= si, f_col, 0.0), axis=0, keepdims=True)
    a_row = ig_ref[...] - c_row
    a_max = jnp.max(a_row, axis=1, keepdims=True)
    g_all = jnp.sum(log_f, axis=1, keepdims=True)
    mem = jnp.zeros((128, 256), F32)
    norm = jnp.zeros((1, 128), F32)
    for b in range(4):
        ti = ri + 128 * b
        col_ref[128 * b : 128 * b + 128, 1:2] = jnp.max(
            jnp.where(si <= ti, a_row, NEG), axis=1, keepdims=True
        )
        a_col = jnp.max(jnp.where(si == ti, a_row, NEG), axis=1, keepdims=True)
        kw = k_ref[128 * b : 128 * b + 128].astype(F32) * jnp.exp(a_col - a_max)
        norm = norm + jnp.sum(kw, axis=0, keepdims=True)
        mem = mem + dg(kw.astype(BF), v_ref[128 * b : 128 * b + 128], TN)
    for h in range(2):
        p1s[16 * h : 16 * h + 16] = mem[:, 128 * h : 128 * h + 128].reshape(16, 8, 128)
    aux = jnp.concatenate(
        [norm, jnp.broadcast_to(g_all, (1, 128)), jnp.broadcast_to(g_all + a_max, (1, 128)), jnp.zeros((1, 128), F32)],
        axis=0,
    )
    auxr[e] = aux
    p1r[e] = p1s[e]

    pl.semaphore_wait(barrier, 37)

    def first(k, _):
        to = (e + k) % 32
        for src, dst, n in ((p1s.at[to], p1r.at[e], 0), (auxr.at[e], auxr.at[e], 1)):
            pltpu.make_async_remote_copy(
                src_ref=src, dst_ref=dst, send_sem=p_send.at[n], recv_sem=p_recv.at[n],
                device_id=(to, t), device_id_type=MESH,
            ).start()
        return 0

    lax.fori_loop(1, 32, first, 0)
    w_in = []
    for d in (1, 2, 3):
        there = (y + d) % 4
        cols = pl.ds(pl.multiple_of(there * 1024, 1024), 1024)
        for n, (src, half) in enumerate(((gate_hbm, 0), (up_hbm, 64))):
            w_in.append(
                send(
                    src.at[:, cols], wt.at[y, pl.ds(half, 64)], w_send.at[2 * d - 2 + n], w_recv.at[2 * d - 2 + n],
                    along("y", d),
                )
            )

    ei = lax.broadcasted_iota(jnp.int32, (256, 128), 1)
    r0, r1 = routes_ref[:, 0:1], routes_ref[:, 1:2]
    hot0, hot1 = (ei == r0).astype(F32), (ei == r1).astype(F32)
    low = (
        lax.broadcasted_iota(jnp.int32, (256, 256), 1) < lax.broadcasted_iota(jnp.int32, (256, 256), 0)
    ).astype(F32).astype(BF)
    cum0 = mm(low, hot0.astype(BF))
    cum1 = mm(low, hot1.astype(BF)) + jnp.sum(hot0, axis=0, keepdims=True)
    s0 = r0.astype(F32) * 32.0 + jnp.sum(hot0 * cum0, axis=1, keepdims=True)
    s1 = r1.astype(F32) * 32.0 + jnp.sum(hot1 * cum1, axis=1, keepdims=True)
    slot = lax.broadcasted_iota(jnp.int32, (256, 1024), 1).astype(F32)
    sel0[...] = (slot == s0).astype(F32).astype(BF)
    sel1[...] = (slot == s1).astype(F32).astype(BF)
    for b in range(4):
        lanes = slice(256 * b, 256 * b + 256)
        both = sel0[:, lanes] + sel1[:, lanes]
        xs[8 * b : 8 * b + 8] = dg(both, x_ref[...], TN).astype(BF).reshape(8, 32, 256)
    own_rows = pl.ds(pl.multiple_of(192 + 32 * c, 32), 32)
    xa[3, x, own_rows, :] = xs[e]

    def dispatch(n):
        for i in range(4 * n, 4 * n + 4):
            at = pl.ds(pl.multiple_of(64 * (i - 4 * n) + 32 * c, 32), 32)
            for other in (1, 0) if i < 15 else (1,):
                to = ((z - HOPS[i] + 16) % 16) * 2 + (c + other) % 2
                pltpu.make_async_remote_copy(
                    src_ref=xs.at[to], dst_ref=xa.at[n, x, at], send_sem=d_send, recv_sem=d_recv.at[n],
                    device_id=(to, t), device_id_type=MESH,
                ).start()

    dispatch(0)
    dispatch(1)

    for b in range(4):
        ti = ri + 128 * b
        w = 128 * b + 128
        at = slice(128 * b, w)
        s = dg(q_ref[at], k_ref[:w], NT) * SCALE
        gate = jnp.exp(jnp.where(si <= ti, a_row, NEG)[:, :w] - col_ref[at, 1:2])
        s = s * gate
        col_ref[at, 2:3] = jnp.sum(s, axis=1, keepdims=True)
        num_ref[at] = mm(s.astype(BF), v_ref[:w])

    def scan_prior():
        bytes_of(p1r.at[pl.ds(0, 31)], p_recv.at[0])
        bytes_of(auxr.at[pl.ds(0, 31)], p_recv.at[1])

        m, n, cc = jnp.full((1, 128), FLOOR, F32), jnp.zeros((1, 128), F32), jnp.zeros((8, 128), F32)
        for k in range(32):
            p2s[k] = cc
            seen[k, 0:1], seen[k, 1:2] = m, n
            if k < 31:
                n2, g2, m2 = auxr[k, 0:1], auxr[k, 1:2], auxr[k, 2:3]
                top = jnp.maximum(g2 + m, m2)
                k1, k2 = jnp.exp(g2 + m - top), jnp.exp(m2 - top)
                m, cc, n = top, k1 * cc + k2 * p1r[k], k1 * n + k2 * n2
        live["pm"], live["pn"] = seen[e, 0:1], seen[e, 1:2]
        p2r[e] = p2s[e]

        def second(k, _):
            to = (e + k) % 32
            pltpu.make_async_remote_copy(
                src_ref=p2s.at[to], dst_ref=p2r.at[e], send_sem=p_send.at[2], recv_sem=p_recv.at[2],
                device_id=(to, t), device_id_type=MESH,
            ).start()
            return 0

        lax.fori_loop(1, 32, second, 0)

    def gather_steps(buf, order, n, cut):
        inner, outer = order
        ci, co = (x, y) if inner == "x" else (y, x)
        ss, rs = ag_send.at[n], ag_recv.at[n]

        def one():
            own = buf.at[co, ci]
            live["g", n] = [send(own, own, ss.at[j], rs.at[j], along(inner, d)) for j, d in enumerate((1, -1 + 4))]

        def two():
            for copy in live["g", n]:
                copy.wait_recv()
            out = []
            for j, d in enumerate((1, 3)):
                part = buf.at[co, (ci - d + 4) % 4, pl.ds(j * cut, cut)]
                out.append(send(part, part, ss.at[2 + j], rs.at[2 + j], along(inner, d)))
            live["g", n] = out

        def three():
            for copy in live["g", n]:
                copy.wait_recv()
            own = buf.at[co]
            live["g", n] = [send(own, own, ss.at[4 + j], rs.at[4 + j], along(outer, d)) for j, d in enumerate((1, 3))]

        def four():
            for copy in live["g", n]:
                copy.wait_recv()
            out = []
            for j, d in enumerate((1, 3)):
                part = buf.at[(co - d + 4) % 4, pl.ds(2 * j, 2)]
                out.append(send(part, part, ss.at[6 + j], rs.at[6 + j], along(outer, d)))
            live["g", n] = out

        def last():
            for copy in live["g", n]:
                copy.wait_recv()

        return one, two, three, four, last

    mix_steps = [gather_steps(mixed.at[h], "xy" if h == 0 else "yx", 4 + h, 128) for h in range(2)]
    hid_steps = [gather_steps(hid.at[n], "xy" if n % 2 == 0 else "yx", n, 32) for n in range(4)]

    def cell_out():
        bytes_of(p2r.at[pl.ds(0, 31)], p_recv.at[2])
        pm, pn = live["pm"][:, 0:1], live["pn"]
        parts = []
        for h in range(2):
            whole = p2r[16 * h : 16 * h + 16].reshape(128, 128)
            hi = whole.astype(BF)
            parts.append((hi, (whole - hi.astype(F32)).astype(BF)))
        for b in range(4):
            at = slice(128 * b, 128 * b + 128)
            qb = q_ref[at]
            c_col, amx, den = col_ref[at, 0:1], col_ref[at, 1:2], col_ref[at, 2:3]
            local, inter = c_col + amx, c_col + pm
            top = jnp.maximum(local, inter)
            f_local, f_inter = jnp.exp(local - top), jnp.exp(inter - top) * SCALE
            qc = jnp.concatenate([mm(qb, hi) + mm(qb, lo) for hi, lo in parts], axis=1)
            num = f_inter * qc + f_local * num_ref[at]
            den = f_inter * jnp.sum(qb.astype(F32) * pn, axis=1, keepdims=True) + f_local * den
            hv = num / jnp.maximum(jnp.abs(den), jnp.exp(-top))
            hv = hv * lax.rsqrt(jnp.mean(hv * hv, axis=1, keepdims=True) + EPS)
            hv = hv * gain_ref[...] * jax.nn.sigmoid(og_ref[at].astype(F32))
            o, i = (y, x) if b < 2 else (x, y)
            mixed[b // 2, o, i, 128 * (b % 2) : 128 * (b % 2) + 128, :] = hv.astype(BF)
        for steps in mix_steps:
            steps[0]()

    def mix_out(h):
        mix_steps[h][4]()
        if h == 0:
            load_mix.wait()
        acc = jnp.zeros((256, 256), F32)
        for o in range(4):
            for i in range(4):
                at = o * 4 + i if h == 0 else i * 4 + o
                acc = acc + mm(mixed[h, o, i], mixw[256 * at : 256 * at + 256])
        out_a[256 * h : 256 * h + 256] = acc.astype(BF)

    def arrive(n):
        k = 8 if n < 3 else 7
        landed = xa.at[n, x, pl.ds(0, 32 * k)]
        bytes_of(landed, d_recv.at[n])
        own = xa.at[n, x]
        live["x", n] = [
            send(own, own, xg_send.at[n, j], xg_recv.at[n, j], along("x", d)) for j, d in enumerate((1, 3))
        ]

    def relay(n):
        for copy in live["x", n]:
            copy.wait_recv()
        out = []
        for j, d in enumerate((1, 3)):
            part = xa.at[n, (x - d + 4) % 4, pl.ds(128 * j, 128)]
            out.append(send(part, part, xg_send.at[n, 2 + j], xg_recv.at[n, 2 + j], along("x", d)))
        live["x", n] = out

    def project(n):
        for copy in live["x", n]:
            copy.wait_recv()
        if n == 0:
            own_g.wait()
            own_u.wait()
            for copy in w_in:
                copy.wait_recv()
        acc = jnp.zeros((512, 256), F32)
        sq = jnp.zeros((16, 256), F32)
        ones = jnp.ones((16, 256), BF)
        for j in range(4):
            xx = xa[n, j]
            w = wt[:, :, 256 * j : 256 * j + 256].reshape(512, 256)
            acc = acc + dg(w, xx, NT)
            wide = xx.astype(F32)
            wide = wide * wide
            hi = wide.astype(BF)
            lo = (wide - hi.astype(F32)).astype(BF)
            sq = sq + dg(ones, hi, NT) + dg(ones, lo, NT)
        hi = sq.astype(BF).astype(F32)
        mid = (sq - hi).astype(BF).astype(F32)
        lo = sq - hi - mid
        row = lax.broadcasted_iota(jnp.int32, (16, 256), 0)
        sq = jnp.where(row == 0, hi, jnp.where(row == 1, mid, jnp.where(row == 2, lo, 0.0))).astype(BF)
        for j in range(4):
            gsend[n, j, 0:128, :] = acc[128 * j : 128 * j + 128].astype(BF)
            gsend[n, j, 128:144, :] = sq
        live["p", n] = [
            send(
                gsend.at[n, (y + d) % 4], grecv.at[n, y], g_send.at[n, d - 1], g_recv.at[n, d - 1], along("y", d)
            )
            for d in (1, 2, 3)
        ]

    def activate(n):
        for copy in live["p", n]:
            copy.wait_recv()
        total = gsend[n, y].astype(F32)
        for d in (1, 2, 3):
            total = total + grecv[n, (y + d) % 4].astype(F32)
        sq = jnp.sum(total[128:144], axis=0, keepdims=True)
        inv = lax.rsqrt(sq / D + EPS)
        g, u = total[0:64] * inv, total[64:128] * inv
        o, i = (y, x) if n % 2 == 0 else (x, y)
        hid[n, o, i] = (g * jax.nn.sigmoid(g) * u).astype(BF)
        hid_steps[n][0]()

    def finish(n):
        hid_steps[n][4]()
        if n == 0:
            load_down.wait()
            for copy in turned:
                copy.wait()
        down = downn if n % 2 == 0 else downt
        res = dg(hid[n].reshape(1024, 256), down[...], TN).astype(BF)
        rows[8 * n : 8 * n + 8] = res.reshape(8, 32, 256)
        for b in range(8):
            i, cs = 4 * n + b // 2, b % 2
            if i < 15:
                to = ((z + HOPS[i]) % 16) * 2 + cs
                pltpu.make_async_remote_copy(
                    src_ref=rows.at[8 * n + b], dst_ref=ret.at[e], send_sem=r_send, recv_sem=r_recv,
                    device_id=(to, t), device_id_type=MESH,
                ).start()
        if n == 3:
            pltpu.make_async_remote_copy(
                src_ref=rows.at[31 - c], dst_ref=ret.at[e], send_sem=r_send, recv_sem=r_recv,
                device_id=(z * 2 + 1 - c, t), device_id_type=MESH,
            ).start()
            ret[e] = rows[30 + c]

    def collect():
        bytes_of(ret.at[pl.ds(0, 31)], r_recv)
        back = ret[...].reshape(1024, 256)
        w0, w1 = rw_ref[:, 0:1], rw_ref[:, 1:2]
        out_b[...] = (mm(sel0[...], back) * w0 + mm(sel1[...], back) * w1).astype(BF)

    plan = [
        (0.0, scan_prior),
        (0.1, lambda: dispatch(2)),
        (0.2, lambda: dispatch(3)),
        (10.0, cell_out),
        (17.0, lambda: [s[1]() for s in mix_steps]),
        (21.0, lambda: [s[2]() for s in mix_steps]),
        (30.0, lambda: [s[3]() for s in mix_steps]),
        (44.0, lambda: mix_out(0)),
        (44.1, lambda: mix_out(1)),
        (100.0, collect),
    ]
    for n, base in enumerate((5.0, 13.0, 23.0, 29.0)):
        stages = [
            arrive, relay, project, activate,
            lambda n: hid_steps[n][1](), lambda n: hid_steps[n][2](), lambda n: hid_steps[n][3](), finish,
        ]
        for j, stage in enumerate(stages):
            plan.append((base + 3.0 * j, functools.partial(stage, n)))
    for _, work in sorted(plan, key=lambda p: p[0]):
        work()

    for copy in sends:
        copy.wait_send()
    bytes_of(p1s.at[pl.ds(0, 31)], p_send.at[0])
    bytes_of(auxr.at[pl.ds(0, 31)], p_send.at[1])
    bytes_of(p2s.at[pl.ds(0, 31)], p_send.at[2])
    bytes_of(xs.at[pl.ds(0, 31)], d_send)
    bytes_of(rows.at[pl.ds(0, 31)], r_send)


def body(q, k, v, ig, fg, og, gain, mixw, xin, routes, rw, gate, up, down):
    vm = pl.BlockSpec(memory_space=pltpu.VMEM)
    hbm = pl.BlockSpec(memory_space=pl.ANY)
    dma = pltpu.SemaphoreType.DMA
    out_a, out_b = pl.pallas_call(
        kernel,
        out_shape=(jax.ShapeDtypeStruct((512, 256), BF), jax.ShapeDtypeStruct((256, 256), BF)),
        in_specs=[vm] * 7 + [hbm] + [vm] * 3 + [hbm] * 3,
        out_specs=(vm, vm),
        scratch_shapes=[
            pltpu.VMEM((4096, 256), BF),
            pltpu.VMEM((1024, 256), BF),
            pltpu.VMEM((1024, 256), BF),
            pltpu.VMEM((4, 128, 1024), BF),
            pltpu.VMEM((32, 32, 256), BF),
            pltpu.VMEM((4, 4, 256, 256), BF),
            pltpu.VMEM((4, 4, 144, 256), BF),
            pltpu.VMEM((4, 4, 144, 256), BF),
            pltpu.VMEM((4, 4, 4, 64, 256), BF),
            pltpu.VMEM((32, 32, 256), BF),
            pltpu.VMEM((32, 32, 256), BF),
            pltpu.VMEM((2, 4, 4, 256, 256), BF),
            pltpu.VMEM((32, 8, 128), F32),
            pltpu.VMEM((32, 8, 128), F32),
            pltpu.VMEM((32, 4, 128), F32),
            pltpu.VMEM((32, 8, 128), F32),
            pltpu.VMEM((32, 8, 128), F32),
            pltpu.VMEM((32, 8, 128), F32),
            pltpu.VMEM((256, 1024), BF),
            pltpu.VMEM((256, 1024), BF),
            pltpu.VMEM((512, 256), F32),
            pltpu.VMEM((512, 128), F32),
            dma((18,)),
            dma((2,)),
            dma((6,)),
            dma((6,)),
            dma((3,)),
            dma((3,)),
            dma,
            dma((4,)),
            dma((4, 4)),
            dma((4, 4)),
            dma((4, 3)),
            dma((4, 3)),
            dma((6, 8)),
            dma((6, 8)),
            dma,
            dma,
        ],
        compiler_params=pltpu.CompilerParams(
            collective_id=0, has_side_effects=True, vmem_limit_bytes=56 * 1024 * 1024
        ),
    )(q, k, v, ig, fg, og, gain.reshape(1, 256), mixw, xin, routes, rw, gate[0], up[0], down[0])
    return out_a, out_b


def solution(mesh):
    in_specs = (
        P("ep", "tp"), P("ep", "tp"), P("ep", "tp"), P("tp", "ep"), P("tp", "ep"), P("ep", "tp"), P("tp"),
        P(None, "tp"), P("ep", "tp"), P("ep", None), P("ep", None), P("ep", "tp", None), P("ep", "tp", None),
        P("ep", None, "tp"),
    )
    return jax.shard_map(
        body, mesh=mesh, in_specs=in_specs, out_specs=(P("ep", "tp"), P("ep", "tp")), check_vma=False
    )
```

```python
import functools

import jax
import jax.numpy as jnp
from jax import lax
from jax.experimental import pallas as pl
from jax.experimental.pallas import tpu as pltpu
from jax.sharding import PartitionSpec as P

MESH = pl.DeviceIdType.MESH
BF, F32 = jnp.bfloat16, jnp.float32
D = 4096
EPS = 1e-6
FLOOR = -1e30
NEG = -3e38
SCALE = 128**-0.5
NC = 8
PER = 16 // NC
S = 1024 // NC
HOPS = [8, 7, 9, 6, 10, 5, 11, 4, 12, 3, 13, 2, 14, 1, 15, 0]
ORDER = [
    (9, 0), (0, 0), (0, 1), (1, 0), (1, 1), (0, 2), (2, 0), (2, 1), (3, 0), (0, 3), (1, 2), (3, 1),
    (0, 4), (4, 0), (1, 3), (0, 5), (2, 2), (4, 1), (0, 6), (0, 7), (1, 4), (5, 0), (2, 3), (5, 1),
    (3, 2), (1, 5), (3, 3), (1, 6), (6, 1), (4, 2), (1, 7), (2, 4), (6, 0), (4, 3), (2, 5), (2, 6),
    (11, 0), (3, 4), (10, 0), (7, 1), (5, 2), (10, 1), (2, 7), (7, 0), (5, 3), (3, 5), (3, 6), (10, 2),
    (4, 4), (3, 7), (8, 0), (6, 3), (10, 3), (8, 1), (6, 2), (4, 5), (4, 6), (4, 7), (12, 0), (7, 2),
    (5, 5), (5, 7), (5, 4), (7, 3), (5, 6), (6, 4), (8, 3), (13, 0), (6, 6), (8, 2), (6, 5), (6, 7),
    (7, 4), (7, 5), (14, 0), (8, 4), (8, 5), (7, 6), (7, 7), (8, 6), (15, 0), (8, 7), (16, 0),
]
NT = (((1,), (1,)), ((), ()))
TN = (((0,), (0,)), ((), ()))


def mm(a, b):
    return jnp.dot(a, b, preferred_element_type=F32)


def dg(a, b, dims):
    return lax.dot_general(a, b, dims, preferred_element_type=F32)


def kernel(
    q_ref, k_ref, v_ref, ig_ref, fg_ref, og_ref, gain_ref, mixw_hbm, x_ref, routes_ref, rw_ref,
    gate_hbm, up_hbm, down_hbm,
    out_a, out_b,
    wm, wr, downn, downt, wt, xs, xa, gsend, grecv, gfar, ggot, gown, qown, hid, rows, ret, mixed, mfar, mgot, msend, mrecv, mown,
    p1s, p1r, auxr, p2s, p2r, seen, sel0, sel1, num_ref, col_ref,
    loc_sem, own_sem, w_send, w_recv, p_send, p_recv, d_send, d_recv,
    xg_send, xg_recv, mw_send, mw_recv, ma_send, ma_recv, mr_send, mr_recv, g_send, g_recv, ag_send, ag_recv, r_send, r_recv,
):
    e, t = lax.axis_index("ep"), lax.axis_index("tp")
    z, c = e // 2, e % 2
    y, x = t // 4, t % 4

    def along(axis, d):
        return (e, y * 4 + (x + d) % 4) if axis == "x" else (e, ((y + d) % 4) * 4 + x)

    def send(src, dst, ss, rs, dev):
        copy = pltpu.make_async_remote_copy(
            src_ref=src, dst_ref=dst, send_sem=ss, recv_sem=rs, device_id=dev, device_id_type=MESH
        )
        copy.start()
        sends.append(copy)
        return copy

    def bytes_of(ref, sem):
        pltpu.make_async_copy(ref, ref, sem).wait()

    sends = []
    live = {}

    def once(name):
        fresh = name not in live
        live[name] = True
        return fresh

    barrier = pltpu.get_barrier_semaphore()

    def hello(k, _):
        pl.semaphore_signal(barrier, inc=1, device_id=((e + k) % 32, t), device_id_type=MESH)
        return 0

    lax.fori_loop(1, 32, hello, 0)
    for axis in "xy":
        for d in (1, 2, 3):
            pl.semaphore_signal(barrier, inc=1, device_id=along(axis, d), device_id_type=MESH)

    own_g = pltpu.make_async_copy(
        gate_hbm.at[:, pl.ds(pl.multiple_of(y * 1024, 1024), 1024)], wt.at[y, pl.ds(0, 64)], own_sem.at[0]
    )
    own_u = pltpu.make_async_copy(
        up_hbm.at[:, pl.ds(pl.multiple_of(y * 1024, 1024), 1024)], wt.at[y, pl.ds(64, 64)], own_sem.at[1]
    )
    own_g.start()
    own_u.start()
    load_mix = pltpu.make_async_copy(mixw_hbm.at[:, x], wm.at[x], loc_sem.at[0])
    load_down = pltpu.make_async_copy(down_hbm, downn, loc_sem.at[1])
    load_mix.start()
    load_down.start()
    turned = []
    for b in range(16):
        copy = pltpu.make_async_copy(
            down_hbm.at[pl.ds(64 * ((b % 4) * 4 + b // 4), 64)], downt.at[pl.ds(64 * b, 64)], loc_sem.at[2 + b]
        )
        copy.start()
        turned.append(copy)


    ei = lax.broadcasted_iota(jnp.int32, (256, 128), 1)
    di = lax.broadcasted_iota(jnp.int32, (256, 256), 0) == lax.broadcasted_iota(jnp.int32, (256, 256), 1)

    def column(row):
        return jnp.sum(jnp.where(di, row, 0.0), axis=1, keepdims=True)

    r0, r1 = (column(routes_ref[j : j + 1].astype(F32)) for j in (0, 1))
    ei = ei.astype(F32)
    hot0, hot1 = (ei == r0).astype(F32), (ei == r1).astype(F32)
    low = (
        lax.broadcasted_iota(jnp.int32, (256, 256), 1) < lax.broadcasted_iota(jnp.int32, (256, 256), 0)
    ).astype(F32).astype(BF)
    cum0 = mm(low, hot0.astype(BF))
    cum1 = mm(low, hot1.astype(BF)) + jnp.sum(hot0, axis=0, keepdims=True)
    s0 = r0 * 32.0 + jnp.sum(hot0 * cum0, axis=1, keepdims=True)
    s1 = r1 * 32.0 + jnp.sum(hot1 * cum1, axis=1, keepdims=True)
    slot = lax.broadcasted_iota(jnp.int32, (256, 1024), 1).astype(F32)
    sel0[...] = (slot == s0).astype(F32).astype(BF)
    sel1[...] = (slot == s1).astype(F32).astype(BF)
    for b in range(4):
        lanes = slice(256 * b, 256 * b + 256)
        both = sel0[:, lanes] + sel1[:, lanes]
        xs[8 * b : 8 * b + 8] = dg(both, x_ref[...], TN).astype(BF).reshape(8, 32, 256)
    own_rows = pl.ds(pl.multiple_of(S - 64 + 32 * c, 32), 32)
    xa[NC - 1, x, own_rows, :] = xs[e]

    def dispatch(n):
        for i in range(PER * n, PER * n + PER):
            at = pl.ds(pl.multiple_of(64 * (i - PER * n) + 32 * c, 32), 32)
            for other in (1, 0) if i < 15 else (1,):
                to = ((z - HOPS[i] + 16) % 16) * 2 + (c + other) % 2
                pltpu.make_async_remote_copy(
                    src_ref=xs.at[to], dst_ref=xa.at[n, x, at], send_sem=d_send, recv_sem=d_recv.at[n],
                    device_id=(to, t), device_id_type=MESH,
                ).start()

    pl.semaphore_wait(barrier, 37)
    for n in range(NC):
        dispatch(n)
    w_in = []
    for d in (1, 2, 3):
        there = (y + d) % 4
        cols = pl.ds(pl.multiple_of(there * 1024, 1024), 1024)
        for n, (src, half) in enumerate(((gate_hbm, 0), (up_hbm, 64))):
            w_in.append(
                send(
                    src.at[:, cols], wt.at[y, pl.ds(half, 64)], w_send.at[2 * d - 2 + n], w_recv.at[2 * d - 2 + n],
                    along("y", d),
                )
            )
    far = [
        send(
            mixw_hbm.at[pl.ds(2 * j, 2), (x + 2) % 4], wr.at[j], mw_send.at[j], mw_recv.at[j], along("x", d)
        )
        for j, d in enumerate((1, 3))
    ]

    f = fg_ref[...]
    log_f = jnp.minimum(f, 0.0) - jnp.log1p(jnp.exp(-jnp.abs(f)))
    si = lax.broadcasted_iota(jnp.int32, (128, 512), 1)
    ri = lax.broadcasted_iota(jnp.int32, (128, 512), 0)
    c_row = jnp.zeros((1, 512), F32)
    for b in range(4):
        ti = ri + 128 * b
        col_ref[128 * b : 128 * b + 128, 0:1] = jnp.sum(
            jnp.where(si <= ti, log_f, 0.0), axis=1, keepdims=True
        )
        f_col = jnp.sum(jnp.where(si == ti, log_f, 0.0), axis=1, keepdims=True)
        c_row = c_row + jnp.sum(jnp.where(ti <= si, f_col, 0.0), axis=0, keepdims=True)
    a_row = ig_ref[...] - c_row
    a_max = jnp.max(a_row, axis=1, keepdims=True)
    g_all = jnp.sum(log_f, axis=1, keepdims=True)
    mem = jnp.zeros((128, 256), F32)
    norm = jnp.zeros((1, 128), F32)
    for b in range(4):
        ti = ri + 128 * b
        col_ref[128 * b : 128 * b + 128, 1:2] = jnp.max(
            jnp.where(si <= ti, a_row, NEG), axis=1, keepdims=True
        )
        a_col = jnp.max(jnp.where(si == ti, a_row, NEG), axis=1, keepdims=True)
        kw = k_ref[128 * b : 128 * b + 128].astype(F32) * jnp.exp(a_col - a_max)
        norm = norm + jnp.sum(kw, axis=0, keepdims=True)
        mem = mem + dg(kw.astype(BF), v_ref[128 * b : 128 * b + 128], TN)
    for h in range(2):
        p1s[16 * h : 16 * h + 16] = mem[:, 128 * h : 128 * h + 128].reshape(16, 8, 128).astype(BF)
    lane = lax.broadcasted_iota(jnp.int32, (1, 128), 1)
    auxr[e, 0:1] = norm
    auxr[e, 1:2] = jnp.where(lane < 64, g_all, g_all + a_max)
    p1r[e] = p1s[e]

    def first(k, _):
        to = (e + k) % 32
        for src, dst, n in ((p1s.at[to], p1r.at[e], 0), (auxr.at[e], auxr.at[e], 1)):
            pltpu.make_async_remote_copy(
                src_ref=src, dst_ref=dst, send_sem=p_send.at[n], recv_sem=p_recv.at[n],
                device_id=(to, t), device_id_type=MESH,
            ).start()
        return 0

    lax.fori_loop(1, 32, first, 0)

    for b in range(4):
        ti = ri + 128 * b
        w = 128 * b + 128
        at = slice(128 * b, w)
        s = dg(q_ref[at], k_ref[:w], NT) * SCALE
        gate = jnp.exp(jnp.where(si <= ti, a_row, NEG)[:, :w] - col_ref[at, 1:2])
        s = s * gate
        col_ref[at, 2:3] = jnp.sum(s, axis=1, keepdims=True)
        num_ref[at] = mm(s.astype(BF), v_ref[:w])

    m_in = []

    def pass_weights():
        for j, d in enumerate((1, 3)):
            far[j].wait_recv()
            m_in.append(
                send(
                    wr.at[j], wm.at[(x - d + 4) % 4, pl.ds(2 * j, 2)], mw_send.at[2 + j], mw_recv.at[2 + j],
                    along("x", d),
                )
            )

    def near_weights(p):
        for j, d in enumerate((1, 3)):
            at = 4 + 2 * p + j
            m_in.append(
                send(mixw_hbm.at[p, (x + d) % 4], wm.at[x, p], mw_send.at[at], mw_recv.at[at], along("x", d))
            )

    def scan_prior():
        bytes_of(p1r.at[pl.ds(0, 31)], p_recv.at[0])
        bytes_of(auxr.at[pl.ds(0, 31)], p_recv.at[1])

        m, n, cc = jnp.full((1, 128), FLOOR, F32), jnp.zeros((1, 128), F32), jnp.zeros((8, 128), F32)
        for k in range(32):
            p2s[k] = cc.astype(BF)
            seen[k, 0:1], seen[k, 1:2] = m, n
            if k < 31:
                n2, g2, m2 = auxr[k, 0:1], auxr[k, 1:2, 0:1], auxr[k, 1:2, 64:65]
                top = jnp.maximum(g2 + m, m2)
                k1, k2 = jnp.exp(g2 + m - top), jnp.exp(m2 - top)
                m, cc, n = top, k1 * cc + k2 * p1r[k].astype(F32), k1 * n + k2 * n2
        live["pm"], live["pn"] = seen[e, 0:1], seen[e, 1:2]
        p2r[e] = p2s[e]

        def second(k, _):
            to = (e + k) % 32
            pltpu.make_async_remote_copy(
                src_ref=p2s.at[to], dst_ref=p2r.at[e], send_sem=p_send.at[2], recv_sem=p_recv.at[2],
                device_id=(to, t), device_id_type=MESH,
            ).start()
            return 0

        lax.fori_loop(1, 32, second, 0)

    def gather_steps(buf, order, n, cut):
        inner, outer = order
        ci, co = (x, y) if inner == "x" else (y, x)
        ss, rs = ag_send.at[n], ag_recv.at[n]

        def one():
            own = buf.at[co, ci]
            live["g", n] = [send(own, own, ss.at[j], rs.at[j], along(inner, d)) for j, d in enumerate((1, -1 + 4))]

        def two():
            for copy in live["g", n]:
                copy.wait_recv()
            out = []
            for j, d in enumerate((1, 3)):
                part = buf.at[co, (ci - d + 4) % 4, pl.ds(j * cut, cut)]
                out.append(send(part, part, ss.at[2 + j], rs.at[2 + j], along(inner, d)))
            live["g", n] = out

        def three():
            for copy in live["g", n]:
                copy.wait_recv()
            own = buf.at[co]
            live["g", n] = [send(own, own, ss.at[4 + j], rs.at[4 + j], along(outer, d)) for j, d in enumerate((1, 3))]

        def four():
            for copy in live["g", n]:
                copy.wait_recv()
            out = []
            for j, d in enumerate((1, 3)):
                part = buf.at[(co - d + 4) % 4, pl.ds(2 * j, 2)]
                out.append(send(part, part, ss.at[6 + j], rs.at[6 + j], along(outer, d)))
            live["g", n] = out

        def last():
            for copy in live["g", n]:
                copy.wait_recv()

        return one, two, three, four, last

    hid_steps = [gather_steps(hid.at[n], "xy" if n % 2 == 0 else "yx", n, 32) for n in range(NC)]

    def cell_out():
        bytes_of(p2r.at[pl.ds(0, 31)], p_recv.at[2])
        pm, pn = live["pm"][:, 0:1], live["pn"]
        parts = []
        for h in range(2):
            parts.append(p2r[16 * h : 16 * h + 16].reshape(128, 128))
        for b in range(4):
            at = slice(128 * b, 128 * b + 128)
            qb = q_ref[at]
            c_col, amx, den = col_ref[at, 0:1], col_ref[at, 1:2], col_ref[at, 2:3]
            local, inter = c_col + amx, c_col + pm
            top = jnp.maximum(local, inter)
            f_local, f_inter = jnp.exp(local - top), jnp.exp(inter - top) * SCALE
            qc = jnp.concatenate([mm(qb, part) for part in parts], axis=1)
            num = f_inter * qc + f_local * num_ref[at]
            den = f_inter * jnp.sum(qb.astype(F32) * pn, axis=1, keepdims=True) + f_local * den
            hv = num / jnp.maximum(jnp.abs(den), jnp.exp(-top))
            hv = hv * lax.rsqrt(jnp.mean(hv * hv, axis=1, keepdims=True) + EPS)
            hv = hv * gain_ref[...] * jax.nn.sigmoid(og_ref[at].astype(F32))
            mixed[y, at, :] = hv.astype(BF)
        own = mixed.at[y]
        live["m"] = [send(own, own, ma_send.at[j], ma_recv.at[j], along("y", d)) for j, d in enumerate((1, 3))]

    def mix_relay():
        for copy in live["m"]:
            copy.wait_recv()
        out = []
        for j, d in enumerate((1, 3)):
            part = mixed.at[(y - d + 4) % 4, pl.ds(256 * j, 256)]
            out.append(send(part, part, ma_send.at[2 + j], ma_recv.at[2 + j], along("y", d)))
        live["m"] = out

    def mix_part():
        for copy in live["m"]:
            copy.wait_recv()
        load_mix.wait()
        for copy in m_in:
            copy.wait_recv()
        for d in (2, 1, 3, 0):
            there = (x + d) % 4
            acc = mm(mixed[0], wm[there, 0])
            for j in range(1, 4):
                acc = acc + mm(mixed[j], wm[there, j])
            if d == 2:
                mfar[...] = acc.astype(BF).reshape(2, 256, 256)
                live["m"] = [
                    send(mfar.at[j], mgot.at[j], mr_send.at[j], mr_recv.at[j], along("x", w))
                    for j, w in enumerate((1, 3))
                ]
            else:
                mown[d] = acc

    def mix_sum():
        for copy in live["m"]:
            copy.wait_recv()
        out = []
        for j, d in enumerate((1, 3)):
            half = slice(256 * j, 256 * j + 256)
            rest = slice(256 - 256 * j, 512 - 256 * j)
            msend[j, half] = (mown[d, half] + mgot[j].astype(F32)).astype(BF)
            msend[j, rest] = mown[d, rest].astype(BF)
            out.append(send(msend.at[j], mrecv.at[j], mr_send.at[2 + j], mr_recv.at[2 + j], along("x", d)))
        live["m"] = out

    def mix_out():
        for copy in live["m"]:
            copy.wait_recv()
        out_a[...] = (mown[0] + mrecv[0].astype(F32) + mrecv[1].astype(F32)).astype(BF)

    def arrive(n):
        k = 2 * PER if n < NC - 1 else 2 * PER - 1
        landed = xa.at[n, x, pl.ds(0, 32 * k)]
        bytes_of(landed, d_recv.at[n])
        own = xa.at[n, x]
        live["x", n] = [
            send(own, own, xg_send.at[n, j], xg_recv.at[n, j], along("x", d)) for j, d in enumerate((1, 3))
        ]

    def relay(n):
        for copy in live["x", n]:
            copy.wait_recv()
        out = []
        for j, d in enumerate((1, 3)):
            part = xa.at[n, (x - d + 4) % 4, pl.ds(S // 2 * j, S // 2)]
            out.append(send(part, part, xg_send.at[n, 2 + j], xg_recv.at[n, 2 + j], along("x", d)))
        live["x", n] = out

    def project(n):
        for copy in live["x", n]:
            copy.wait_recv()
        if once("wt"):
            own_g.wait()
            own_u.wait()
            for copy in w_in:
                copy.wait_recv()
        acc = jnp.zeros((512, S), F32)
        sq = jnp.zeros((16, S), F32)
        ones = jnp.ones((16, 256), BF)
        for j in range(4):
            xx = xa[n, j]
            w = wt[:, :, 256 * j : 256 * j + 256].reshape(512, 256)
            acc = acc + dg(w, xx, NT)
            wide = xx.astype(F32)
            wide = wide * wide
            hi = wide.astype(BF)
            lo = (wide - hi.astype(F32)).astype(BF)
            sq = sq + dg(ones, hi, NT) + dg(ones, lo, NT)
        gown[n] = acc.reshape(4, 128, S)
        qown[n] = sq
        gfar[n, 0:128] = gown[n, (y + 2) % 4].astype(BF)
        gfar[n, 128:144] = in_three(sq)
        live["p", n] = [
            send(
                gfar.at[n, pl.ds(64 * j, 64 + 16 * j)], ggot.at[n, pl.ds(64 * j, 64 + 16 * j)],
                g_send.at[n, j], g_recv.at[n, j], along("y", d),
            )
            for j, d in enumerate((1, 3))
        ]

    def in_three(sq):
        hi = sq.astype(BF).astype(F32)
        mid = (sq - hi).astype(BF).astype(F32)
        row = lax.broadcasted_iota(jnp.int32, (16, S), 0)
        parts = jnp.where(row == 0, hi, jnp.where(row == 1, mid, jnp.where(row == 2, sq - hi - mid, 0.0)))
        return parts.astype(BF)

    def partial_sum(n):
        for copy in live["p", n]:
            copy.wait_recv()
        sq = qown[n]
        gsend[n, 0, 0:64] = (gown[n, (y + 1) % 4, 0:64] + ggot[n, 0:64].astype(F32)).astype(BF)
        gsend[n, 0, 64:128] = gown[n, (y + 1) % 4, 64:128].astype(BF)
        gsend[n, 0, 128:144] = in_three(sq)
        gsend[n, 1, 0:64] = gown[n, (y + 3) % 4, 0:64].astype(BF)
        gsend[n, 1, 64:128] = (gown[n, (y + 3) % 4, 64:128] + ggot[n, 64:128].astype(F32)).astype(BF)
        gsend[n, 1, 128:144] = in_three(sq + jnp.sum(ggot[n, 128:144].astype(F32), axis=0, keepdims=True))
        live["p", n] = [
            send(gsend.at[n, j], grecv.at[n, j], g_send.at[n, 2 + j], g_recv.at[n, 2 + j], along("y", d))
            for j, d in enumerate((1, 3))
        ]

    def activate(n):
        for copy in live["p", n]:
            copy.wait_recv()
        total = gown[n, y] + grecv[n, 0, 0:128].astype(F32) + grecv[n, 1, 0:128].astype(F32)
        sq = qown[n, 0:1] + jnp.sum(
            grecv[n, 0, 128:144].astype(F32) + grecv[n, 1, 128:144].astype(F32), axis=0, keepdims=True
        )
        inv = lax.rsqrt(sq / D + EPS)
        g, u = total[0:64] * inv, total[64:128] * inv
        o, i = (y, x) if n % 2 == 0 else (x, y)
        hid[n, o, i] = (g * jax.nn.sigmoid(g) * u).astype(BF)
        hid_steps[n][0]()

    def finish(n):
        hid_steps[n][4]()
        if once("down"):
            load_down.wait()
            for copy in turned:
                copy.wait()
        down = downn if n % 2 == 0 else downt
        res = dg(hid[n].reshape(1024, S), down[...], TN).astype(BF)
        rows[2 * PER * n : 2 * PER * n + 2 * PER] = res.reshape(2 * PER, 32, 256)
        for b in range(2 * PER):
            i, cs = PER * n + b // 2, b % 2
            if i < 15:
                to = ((z + HOPS[i]) % 16) * 2 + cs
                pltpu.make_async_remote_copy(
                    src_ref=rows.at[2 * PER * n + b], dst_ref=ret.at[e], send_sem=r_send, recv_sem=r_recv,
                    device_id=(to, t), device_id_type=MESH,
                ).start()
        if n == NC - 1:
            pltpu.make_async_remote_copy(
                src_ref=rows.at[31 - c], dst_ref=ret.at[e], send_sem=r_send, recv_sem=r_recv,
                device_id=(z * 2 + 1 - c, t), device_id_type=MESH,
            ).start()
            ret[e] = rows[30 + c]

    def collect():
        bytes_of(ret.at[pl.ds(0, 31)], r_recv)
        back = ret[...].reshape(1024, 256)
        w0, w1 = column(rw_ref[0:1]), column(rw_ref[1:2])
        out_b[...] = (mm(sel0[...], back) * w0 + mm(sel1[...], back) * w1).astype(BF)

    stages = [
        arrive, relay, project, partial_sum, activate,
        lambda n: hid_steps[n][1](), lambda n: hid_steps[n][2](), lambda n: hid_steps[n][3](), finish,
        lambda n: pass_weights(), near_weights, lambda n: scan_prior(), lambda n: cell_out(),
        lambda n: mix_relay(), lambda n: mix_part(), lambda n: mix_sum(), lambda n: mix_out(),
    ]
    for which, n in ORDER:
        stages[which](n)
    collect()

    for copy in sends:
        copy.wait_send()
    bytes_of(p1s.at[pl.ds(0, 31)], p_send.at[0])
    bytes_of(auxr.at[pl.ds(0, 31)], p_send.at[1])
    bytes_of(p2s.at[pl.ds(0, 31)], p_send.at[2])
    bytes_of(xs.at[pl.ds(0, 31)], d_send)
    bytes_of(rows.at[pl.ds(0, 31)], r_send)


def body(q, k, v, ig, fg, og, gain, mixw, xin, routes, rw, gate, up, down):
    vm = pl.BlockSpec(memory_space=pltpu.VMEM)
    hbm = pl.BlockSpec(memory_space=pl.ANY)
    dma = pltpu.SemaphoreType.DMA
    out_a, out_b = pl.pallas_call(
        kernel,
        out_shape=(jax.ShapeDtypeStruct((512, 256), BF), jax.ShapeDtypeStruct((256, 256), BF)),
        in_specs=[vm] * 7 + [hbm] + [vm] * 3 + [hbm] * 3,
        out_specs=(vm, vm),
        scratch_shapes=[
            pltpu.VMEM((4, 4, 256, 256), BF),
            pltpu.VMEM((2, 2, 256, 256), BF),
            pltpu.VMEM((1024, 256), BF),
            pltpu.VMEM((1024, 256), BF),
            pltpu.VMEM((4, 128, 1024), BF),
            pltpu.VMEM((32, 32, 256), BF),
            pltpu.VMEM((NC, 4, S, 256), BF),
            pltpu.VMEM((NC, 2, 144, S), BF),
            pltpu.VMEM((NC, 2, 144, S), BF),
            pltpu.VMEM((NC, 144, S), BF),
            pltpu.VMEM((NC, 144, S), BF),
            pltpu.VMEM((NC, 4, 128, S), F32),
            pltpu.VMEM((NC, 16, S), F32),
            pltpu.VMEM((NC, 4, 4, 64, S), BF),
            pltpu.VMEM((32, 32, 256), BF),
            pltpu.VMEM((32, 32, 256), BF),
            pltpu.VMEM((4, 512, 256), BF),
            pltpu.VMEM((2, 256, 256), BF),
            pltpu.VMEM((2, 256, 256), BF),
            pltpu.VMEM((2, 512, 256), BF),
            pltpu.VMEM((2, 512, 256), BF),
            pltpu.VMEM((4, 512, 256), F32),
            pltpu.VMEM((32, 8, 128), BF),
            pltpu.VMEM((32, 8, 128), BF),
            pltpu.VMEM((32, 2, 128), F32),
            pltpu.VMEM((32, 8, 128), BF),
            pltpu.VMEM((32, 8, 128), BF),
            pltpu.VMEM((32, 8, 128), F32),
            pltpu.VMEM((256, 1024), BF),
            pltpu.VMEM((256, 1024), BF),
            pltpu.VMEM((512, 256), F32),
            pltpu.VMEM((512, 128), F32),
            dma((18,)),
            dma((2,)),
            dma((6,)),
            dma((6,)),
            dma((3,)),
            dma((3,)),
            dma,
            dma((NC,)),
            dma((NC, 4)),
            dma((NC, 4)),
            dma((12,)),
            dma((12,)),
            dma((4,)),
            dma((4,)),
            dma((4,)),
            dma((4,)),
            dma((NC, 4)),
            dma((NC, 4)),
            dma((NC, 8)),
            dma((NC, 8)),
            dma,
            dma,
        ],
        compiler_params=pltpu.CompilerParams(
            collective_id=0, has_side_effects=True, vmem_limit_bytes=56 * 1024 * 1024
        ),
    )(q, k, v, ig, fg, og, gain.reshape(1, 256), mixw.reshape(4, 4, 256, 256), xin, routes.T, rw.T, gate[0], up[0], down[0])
    return out_a, out_b


def solution(mesh):
    in_specs = (
        P("ep", "tp"), P("ep", "tp"), P("ep", "tp"), P("tp", "ep"), P("tp", "ep"), P("ep", "tp"), P("tp"),
        P(None, "tp"), P("ep", "tp"), P("ep", None), P("ep", None), P("ep", "tp", None), P("ep", "tp", None),
        P("ep", None, "tp"),
    )
    return jax.shard_map(
        body, mesh=mesh, in_specs=in_specs, out_specs=(P("ep", "tp"), P("ep", "tp")), check_vma=False
    )
```

```python
import functools

import jax
import jax.numpy as jnp
from jax import lax
from jax.experimental import pallas as pl
from jax.experimental.pallas import tpu as pltpu
from jax.sharding import PartitionSpec as P

MESH = pl.DeviceIdType.MESH
BF, F32 = jnp.bfloat16, jnp.float32
D = 4096
EPS = 1e-6
FLOOR = -1e30
NEG = -3e38
SCALE = 128**-0.5
NC = 8
PER = 16 // NC
S = 1024 // NC
HOPS = [3, 13, 2, 14, 4, 12, 7, 9, 6, 10, 1, 15, 5, 11, 8, 0]
X_FIRST = [1, 0, 1, 0, 1, 1, 1, 0]
ORDER = [
    (17, 2), (18, 0), (17, 5), (17, 4), (19, 0), (17, 7), (10, 3), (0, 2), (10, 2), (17, 1), (17, 3), (0, 5),
    (17, 0), (0, 4), (1, 2), (1, 4), (1, 5), (0, 7), (2, 2), (0, 1), (17, 6), (2, 4), (3, 2), (1, 7),
    (20, 0), (3, 4), (1, 1), (2, 5), (0, 3), (0, 0), (2, 7), (4, 4), (4, 2), (1, 3), (3, 5), (0, 6),
    (3, 7), (5, 4), (5, 2), (1, 0), (2, 1), (2, 3), (4, 7), (6, 4), (1, 6), (9, 0), (6, 2), (11, 0),
    (3, 3), (4, 5), (5, 7), (3, 1), (7, 4), (2, 6), (2, 0), (6, 7), (4, 3), (7, 2), (10, 0), (8, 4),
    (4, 1), (3, 6), (3, 0), (5, 3), (12, 0), (7, 7), (4, 6), (5, 5), (4, 0), (8, 2), (5, 6), (8, 7),
    (5, 1), (6, 3), (10, 1), (6, 6), (7, 3), (13, 0), (6, 1), (6, 5), (5, 0), (7, 6), (8, 3), (7, 1),
    (6, 0), (14, 0), (7, 5), (8, 6), (7, 0), (15, 0), (8, 0), (8, 1), (8, 5), (16, 0),
]
NT = (((1,), (1,)), ((), ()))
TN = (((0,), (0,)), ((), ()))


def mm(a, b):
    return jnp.dot(a, b, preferred_element_type=F32)


def dg(a, b, dims):
    return lax.dot_general(a, b, dims, preferred_element_type=F32)


def kernel(
    q_hbm, k_hbm, v_hbm, ig_hbm, fg_hbm, og_hbm, gain_hbm, mixw_hbm, x_hbm, routes_hbm, rw_hbm,
    gate_hbm, up_hbm, down_hbm,
    far_a, far_b,
    q_ref, k_ref, v_ref, ig_ref, fg_ref, og_ref, gain_ref, x_ref, routes_ref, rw_ref, out_a, out_b,
    wm, wr, downn, downt, wt, xs, xa, gsend, grecv, gfar, ggot, gown, qown, hid, rows, ret, mixed, mfar, mgot, msend, mrecv, mown,
    p1s, p1r, p2s, p2r, seen, sel0, sel1, num_ref, col_ref,
    in_sem, out_sem, loc_sem, own_sem, w_send, w_recv, p_send, p_recv, d_send, d_recv,
    xg_send, xg_recv, far_send, far_recv, mw_send, mw_recv, ma_send, ma_recv, mr_send, mr_recv, g_send, g_recv,
    ag_near, ag_wide, ag_recv, r_send, r_recv,
):
    e, t = lax.axis_index("ep"), lax.axis_index("tp")
    z, c = e // 2, e % 2
    y, x = t // 4, t % 4

    def along(axis, d):
        return (e, y * 4 + (x + d) % 4) if axis == "x" else (e, ((y + d) % 4) * 4 + x)

    def send(src, dst, ss, rs, dev):
        copy = pltpu.make_async_remote_copy(
            src_ref=src, dst_ref=dst, send_sem=ss, recv_sem=rs, device_id=dev, device_id_type=MESH
        )
        copy.start()

    def bytes_of(ref, sem):
        pltpu.make_async_copy(ref, ref, sem).wait()

    live = {}

    def once(name):
        fresh = name not in live
        live[name] = True
        return fresh

    barrier = pltpu.get_barrier_semaphore()

    def hello(k, _):
        pl.semaphore_signal(barrier, inc=1, device_id=((e + k) % 32, t), device_id_type=MESH)
        return 0

    lax.fori_loop(1, 32, hello, 0)
    for axis in "xy":
        for d in (1, 2, 3):
            pl.semaphore_signal(barrier, inc=1, device_id=along(axis, d), device_id_type=MESH)

    arriving = []
    for j, (src, dst) in enumerate((
        (routes_hbm, routes_ref), (x_hbm, x_ref), (fg_hbm, fg_ref), (ig_hbm, ig_ref), (k_hbm, k_ref), (v_hbm, v_ref),
        (q_hbm, q_ref), (og_hbm, og_ref), (gain_hbm, gain_ref), (rw_hbm, rw_ref),
    )):
        copy = pltpu.make_async_copy(src, dst, in_sem.at[j])
        copy.start()
        arriving.append(copy)

    own_g = pltpu.make_async_copy(
        gate_hbm.at[:, pl.ds(pl.multiple_of(y * 1024, 1024), 1024)], wt.at[y, pl.ds(0, 64)], own_sem
    )
    own_u = pltpu.make_async_copy(
        up_hbm.at[:, pl.ds(pl.multiple_of(y * 1024, 1024), 1024)], wt.at[y, pl.ds(64, 64)], own_sem
    )
    own_g.start()
    own_u.start()
    load_mix = pltpu.make_async_copy(mixw_hbm.at[:, x], wm.at[x], loc_sem.at[0])
    load_down = pltpu.make_async_copy(down_hbm, downn, loc_sem.at[1])
    load_mix.start()
    load_down.start()
    turned = []
    for b in range(16 if not all(X_FIRST) else 0):
        copy = pltpu.make_async_copy(
            down_hbm.at[pl.ds(64 * ((b % 4) * 4 + b // 4), 64)], downt.at[pl.ds(64 * b, 64)], loc_sem.at[2]
        )
        copy.start()
        turned.append(copy)


    arriving[0].wait()
    ei = lax.broadcasted_iota(jnp.int32, (256, 128), 1)
    di = lax.broadcasted_iota(jnp.int32, (256, 256), 0) == lax.broadcasted_iota(jnp.int32, (256, 256), 1)

    def column(row):
        return jnp.sum(jnp.where(di, row, 0.0), axis=1, keepdims=True)

    r0, r1 = (column(routes_ref[j : j + 1].astype(F32)) for j in (0, 1))
    ei = ei.astype(F32)
    hot0, hot1 = (ei == r0).astype(F32), (ei == r1).astype(F32)
    low = (
        lax.broadcasted_iota(jnp.int32, (256, 256), 1) < lax.broadcasted_iota(jnp.int32, (256, 256), 0)
    ).astype(F32).astype(BF)
    cum0 = mm(low, hot0.astype(BF))
    cum1 = mm(low, hot1.astype(BF)) + jnp.sum(hot0, axis=0, keepdims=True)
    s0 = r0 * 32.0 + jnp.sum(hot0 * cum0, axis=1, keepdims=True)
    s1 = r1 * 32.0 + jnp.sum(hot1 * cum1, axis=1, keepdims=True)
    arriving[1].wait()
    slot = lax.broadcasted_iota(jnp.int32, (256, 1024), 1).astype(F32)
    sel0[...] = (slot == s0).astype(F32).astype(BF)
    sel1[...] = (slot == s1).astype(F32).astype(BF)
    for b in range(4):
        lanes = slice(256 * b, 256 * b + 256)
        both = sel0[:, lanes] + sel1[:, lanes]
        xs[8 * b : 8 * b + 8] = dg(both, x_ref[...], TN).astype(BF).reshape(8, 32, 256)
    own_rows = pl.ds(pl.multiple_of(S - 64 + 32 * c, 32), 32)
    xa[NC - 1, x, own_rows, :] = xs[e]

    def dispatch(n):
        for i in range(PER * n, PER * n + PER):
            at = pl.ds(pl.multiple_of(64 * (i - PER * n) + 32 * c, 32), 32)
            for other in (1, 0) if i < 15 else (1,):
                to = ((z - HOPS[i] + 16) % 16) * 2 + (c + other) % 2
                pltpu.make_async_remote_copy(
                    src_ref=xs.at[to], dst_ref=xa.at[n, x, at], send_sem=d_send, recv_sem=d_recv.at[n],
                    device_id=(to, t), device_id_type=MESH,
                ).start()

    pl.semaphore_wait(barrier, 37)
    def weights_out():
        for d in (1, 2, 3):
            cols = pl.ds(pl.multiple_of((y + d) % 4 * 1024, 1024), 1024)
            for src, half in ((gate_hbm, 0), (up_hbm, 64)):
                send(src.at[:, cols], wt.at[y, pl.ds(half, 64)], w_send, w_recv, along("y", d))

    def far_weights():
        for j, d in enumerate((1, 3)):
            send(mixw_hbm.at[pl.ds(2 * j, 2), (x + 2) % 4], wr.at[j], far_send, far_recv, along("x", d))

    si = lax.broadcasted_iota(jnp.int32, (128, 512), 1)
    ri = lax.broadcasted_iota(jnp.int32, (128, 512), 0)

    def states():
        for copy in arriving[2:6]:
            copy.wait()
        f = fg_ref[...]
        log_f = jnp.minimum(f, 0.0) - jnp.log1p(jnp.exp(-jnp.abs(f)))
        c_row = jnp.zeros((1, 512), F32)
        for b in range(4):
            ti = ri + 128 * b
            col_ref[128 * b : 128 * b + 128, 0:1] = jnp.sum(
                jnp.where(si <= ti, log_f, 0.0), axis=1, keepdims=True
            )
            f_col = jnp.sum(jnp.where(si == ti, log_f, 0.0), axis=1, keepdims=True)
            c_row = c_row + jnp.sum(jnp.where(ti <= si, f_col, 0.0), axis=0, keepdims=True)
        a_row = ig_ref[...] - c_row
        a_max = jnp.max(a_row, axis=1, keepdims=True)
        g_all = jnp.sum(log_f, axis=1, keepdims=True)
        mem = jnp.zeros((128, 256), F32)
        norm = jnp.zeros((1, 128), F32)
        for b in range(4):
            ti = ri + 128 * b
            col_ref[128 * b : 128 * b + 128, 1:2] = jnp.max(
                jnp.where(si <= ti, a_row, NEG), axis=1, keepdims=True
            )
            a_col = jnp.max(jnp.where(si == ti, a_row, NEG), axis=1, keepdims=True)
            kw = k_ref[128 * b : 128 * b + 128].astype(F32) * jnp.exp(a_col - a_max)
            norm = norm + jnp.sum(kw, axis=0, keepdims=True)
            mem = mem + dg(kw.astype(BF), v_ref[128 * b : 128 * b + 128], TN)
        lane = lax.broadcasted_iota(jnp.int32, (1, 128), 1)
        both = jnp.where(lane < 64, g_all, g_all + a_max)
        row = lax.broadcasted_iota(jnp.int32, (8, 128), 0)
        aux = jnp.zeros((8, 128), F32)
        for j, rest in enumerate((norm, both)):
            for n in range(3):
                part = rest.astype(BF).astype(F32)
                aux = jnp.where(row == 3 * j + n, part, aux)
                rest = rest - part
        for h in range(2):
            tiles = mem[:, 128 * h : 128 * h + 128].reshape(16, 8, 128)
            p1s[16 * h : 16 * h + 16] = jnp.concatenate(
                [tiles, jnp.broadcast_to(aux[None], (16, 8, 128))], axis=1
            ).astype(BF)
        p1r[e] = p1s[e]
        live["a_row"] = a_row

        def first(k, _):
            to = (e + k) % 32
            pltpu.make_async_remote_copy(
                src_ref=p1s.at[to], dst_ref=p1r.at[e], send_sem=p_send.at[0], recv_sem=p_recv.at[0],
                device_id=(to, t), device_id_type=MESH,
            ).start()
            return 0

        lax.fori_loop(1, 32, first, 0)

    def inside():
        a_row = live["a_row"]
        arriving[6].wait()
        for b in range(4):
            ti = ri + 128 * b
            w = 128 * b + 128
            at = slice(128 * b, w)
            s = dg(q_ref[at], k_ref[:w], NT) * SCALE
            gate = jnp.exp(jnp.where(si <= ti, a_row, NEG)[:, :w] - col_ref[at, 1:2])
            s = s * gate
            col_ref[at, 2:3] = jnp.sum(s, axis=1, keepdims=True)
            num_ref[at] = mm(s.astype(BF), v_ref[:w])

    def pass_weights():
        if "a_row" in live and once("inside"):
            inside()
        bytes_of(wr, far_recv)
        for j, d in enumerate((1, 3)):
            send(wr.at[j], wm.at[(x - d + 4) % 4, pl.ds(2 * j, 2)], mw_send, mw_recv, along("x", d))

    def near_weights(p):
        for d in (1, 3):
            send(mixw_hbm.at[p, (x + d) % 4], wm.at[x, p], mw_send, mw_recv, along("x", d))

    def scan_prior():
        if once("inside"):
            inside()
        bytes_of(p1r.at[pl.ds(0, 31)], p_recv.at[0])

        m, n, cc = jnp.full((1, 128), FLOOR, F32), jnp.zeros((1, 128), F32), jnp.zeros((8, 128), F32)
        for k in range(32):
            p2s[k] = cc.astype(BF)
            seen[k, 0:1], seen[k, 1:2] = m, n
            if k < 31:
                got = p1r[k].astype(F32)
                n2 = got[8:9] + got[9:10] + got[10:11]
                both = got[11:12] + got[12:13] + got[13:14]
                g2, m2 = both[:, 0:1], both[:, 64:65]
                top = jnp.maximum(g2 + m, m2)
                k1, k2 = jnp.exp(g2 + m - top), jnp.exp(m2 - top)
                m, cc, n = top, k1 * cc + k2 * got[0:8], k1 * n + k2 * n2
        live["pm"], live["pn"] = seen[e, 0:1], seen[e, 1:2]
        p2r[e] = p2s[e]

        def second(k, _):
            to = (e + k) % 32
            pltpu.make_async_remote_copy(
                src_ref=p2s.at[to], dst_ref=p2r.at[e], send_sem=p_send.at[1], recv_sem=p_recv.at[1],
                device_id=(to, t), device_id_type=MESH,
            ).start()
            return 0

        lax.fori_loop(1, 32, second, 0)

    def gather_steps(buf, order, n, cut):
        inner, outer = order
        ci, co = (x, y) if inner == "x" else (y, x)
        near, wide, rs = ag_near, ag_wide, ag_recv

        def one():
            own = buf.at[co, ci]
            for d in (1, 3):
                send(own, own, near, rs.at[n, 0], along(inner, d))

        def two():
            bytes_of(buf.at[co, pl.ds(0, 2)], rs.at[n, 0])
            for j, d in enumerate((1, 3)):
                part = buf.at[co, (ci - d + 4) % 4, pl.ds(j * cut, cut)]
                send(part, part, near, rs.at[n, 1], along(inner, d))

        def three():
            bytes_of(buf.at[co, 0], rs.at[n, 1])
            own = buf.at[co]
            for d in (1, 3):
                send(own, own, wide, rs.at[n, 2], along(outer, d))

        def four():
            bytes_of(buf.at[pl.ds(0, 2)], rs.at[n, 2])
            for j, d in enumerate((1, 3)):
                part = buf.at[(co - d + 4) % 4, pl.ds(2 * j, 2)]
                send(part, part, wide, rs.at[n, 3], along(outer, d))

        def last():
            bytes_of(buf.at[0], rs.at[n, 3])

        return one, two, three, four, last

    hid_steps = [gather_steps(hid.at[n], "xy" if X_FIRST[n] else "yx", n, 32) for n in range(NC)]

    def cell_out():
        for copy in arriving[7:9]:
            copy.wait()
        bytes_of(p2r.at[pl.ds(0, 31)], p_recv.at[1])
        pm, pn = live["pm"][:, 0:1], live["pn"]
        parts = []
        for h in range(2):
            parts.append(p2r[16 * h : 16 * h + 16].reshape(128, 128))
        for b in range(4):
            at = slice(128 * b, 128 * b + 128)
            qb = q_ref[at]
            c_col, amx, den = col_ref[at, 0:1], col_ref[at, 1:2], col_ref[at, 2:3]
            local, inter = c_col + amx, c_col + pm
            top = jnp.maximum(local, inter)
            f_local, f_inter = jnp.exp(local - top), jnp.exp(inter - top) * SCALE
            qc = jnp.concatenate([mm(qb, part) for part in parts], axis=1)
            num = f_inter * qc + f_local * num_ref[at]
            den = f_inter * jnp.sum(qb.astype(F32) * pn, axis=1, keepdims=True) + f_local * den
            hv = num / jnp.maximum(jnp.abs(den), jnp.exp(-top))
            hv = hv * lax.rsqrt(jnp.mean(hv * hv, axis=1, keepdims=True) + EPS)
            hv = hv * gain_ref[...] * jax.nn.sigmoid(og_ref[at].astype(F32))
            mixed[y, at, :] = hv.astype(BF)
        own = mixed.at[y]
        for d in (1, 3):
            send(own, own, ma_send, ma_recv.at[0], along("y", d))

    def mix_relay():
        bytes_of(mixed.at[pl.ds(0, 2)], ma_recv.at[0])
        for j, d in enumerate((1, 3)):
            part = mixed.at[(y - d + 4) % 4, pl.ds(256 * j, 256)]
            send(part, part, ma_send, ma_recv.at[1], along("y", d))

    def mix_part():
        bytes_of(mixed.at[0], ma_recv.at[1])
        load_mix.wait()
        bytes_of(wm.at[pl.ds(0, 3)], mw_recv)
        for d in (2, 1, 3, 0):
            there = (x + d) % 4
            acc = mm(mixed[0], wm[there, 0])
            for j in range(1, 4):
                acc = acc + mm(mixed[j], wm[there, j])
            if d == 2:
                mfar[...] = acc.astype(BF).reshape(2, 256, 256)
                for j, w in enumerate((1, 3)):
                    send(mfar.at[j], mgot.at[j], mr_send.at[0], mr_recv.at[0], along("x", w))
            else:
                mown[d] = acc

    def mix_sum():
        bytes_of(mgot, mr_recv.at[0])
        for j, d in enumerate((1, 3)):
            half = slice(256 * j, 256 * j + 256)
            rest = slice(256 - 256 * j, 512 - 256 * j)
            msend[j, half] = (mown[d, half] + mgot[j].astype(F32)).astype(BF)
            msend[j, rest] = mown[d, rest].astype(BF)
            send(msend.at[j], mrecv.at[j], mr_send.at[1], mr_recv.at[1], along("x", d))

    def mix_out():
        bytes_of(mrecv, mr_recv.at[1])
        out_a[...] = (mown[0] + mrecv[0].astype(F32) + mrecv[1].astype(F32)).astype(BF)
        pltpu.make_async_copy(out_a, far_a, out_sem.at[0]).start()

    def arrive(n):
        k = 2 * PER if n < NC - 1 else 2 * PER - 1
        landed = xa.at[n, x, pl.ds(0, 32 * k)]
        bytes_of(landed, d_recv.at[n])
        own = xa.at[n, x]
        for d in (1, 3):
            send(own, own, xg_send, xg_recv.at[n, 0], along("x", d))

    def relay(n):
        bytes_of(xa.at[n, pl.ds(0, 2)], xg_recv.at[n, 0])
        for j, d in enumerate((1, 3)):
            part = xa.at[n, (x - d + 4) % 4, pl.ds(S // 2 * j, S // 2)]
            send(part, part, xg_send, xg_recv.at[n, 1], along("x", d))

    def project(n):
        bytes_of(xa.at[n, 0], xg_recv.at[n, 1])
        if once("wt"):
            bytes_of(wt.at[y], own_sem)
            bytes_of(wt.at[pl.ds(0, 3)], w_recv)
        acc = jnp.zeros((512, S), F32)
        sq = jnp.zeros((16, S), F32)
        ones = jnp.ones((16, 256), BF)
        for j in range(4):
            xx = xa[n, j]
            w = wt[:, :, 256 * j : 256 * j + 256].reshape(512, 256)
            acc = acc + dg(w, xx, NT)
            wide = xx.astype(F32)
            wide = wide * wide
            hi = wide.astype(BF)
            lo = (wide - hi.astype(F32)).astype(BF)
            sq = sq + dg(ones, hi, NT) + dg(ones, lo, NT)
        gown[n] = acc.reshape(4, 128, S)
        qown[n] = sq
        gfar[n, 0:128] = gown[n, (y + 2) % 4].astype(BF)
        gfar[n, 128:144] = in_three(sq)
        for j, d in enumerate((1, 3)):
            at = pl.ds(64 * j, 64 + 16 * j)
            send(gfar.at[n, at], ggot.at[n, at], g_send.at[0], g_recv.at[n, 0], along("y", d))

    def in_three(sq):
        hi = sq.astype(BF).astype(F32)
        mid = (sq - hi).astype(BF).astype(F32)
        row = lax.broadcasted_iota(jnp.int32, (16, S), 0)
        parts = jnp.where(row == 0, hi, jnp.where(row == 1, mid, jnp.where(row == 2, sq - hi - mid, 0.0)))
        return parts.astype(BF)

    def partial_sum(n):
        bytes_of(ggot.at[n], g_recv.at[n, 0])
        sq = qown[n]
        gsend[n, 0, 0:64] = (gown[n, (y + 1) % 4, 0:64] + ggot[n, 0:64].astype(F32)).astype(BF)
        gsend[n, 0, 64:128] = gown[n, (y + 1) % 4, 64:128].astype(BF)
        gsend[n, 0, 128:144] = in_three(sq)
        gsend[n, 1, 0:64] = gown[n, (y + 3) % 4, 0:64].astype(BF)
        gsend[n, 1, 64:128] = (gown[n, (y + 3) % 4, 64:128] + ggot[n, 64:128].astype(F32)).astype(BF)
        gsend[n, 1, 128:144] = in_three(sq + jnp.sum(ggot[n, 128:144].astype(F32), axis=0, keepdims=True))
        for j, d in enumerate((1, 3)):
            send(gsend.at[n, j], grecv.at[n, j], g_send.at[1], g_recv.at[n, 1], along("y", d))

    def activate(n):
        bytes_of(grecv.at[n], g_recv.at[n, 1])
        total = gown[n, y] + grecv[n, 0, 0:128].astype(F32) + grecv[n, 1, 0:128].astype(F32)
        sq = qown[n, 0:1] + jnp.sum(
            grecv[n, 0, 128:144].astype(F32) + grecv[n, 1, 128:144].astype(F32), axis=0, keepdims=True
        )
        inv = lax.rsqrt(sq / D + EPS)
        g, u = total[0:64] * inv, total[64:128] * inv
        o, i = (y, x) if X_FIRST[n] else (x, y)
        hid[n, o, i] = (g * jax.nn.sigmoid(g) * u).astype(BF)
        hid_steps[n][0]()

    def finish(n):
        hid_steps[n][4]()
        if once("down"):
            load_down.wait()
            if turned:
                bytes_of(downt, loc_sem.at[2])
        down = downn if X_FIRST[n] else downt
        res = dg(hid[n].reshape(1024, S), down[...], TN).astype(BF)
        rows[2 * PER * n : 2 * PER * n + 2 * PER] = res.reshape(2 * PER, 32, 256)
        for b in range(2 * PER):
            i, cs = PER * n + b // 2, b % 2
            if i < 15:
                to = ((z + HOPS[i]) % 16) * 2 + cs
                pltpu.make_async_remote_copy(
                    src_ref=rows.at[2 * PER * n + b], dst_ref=ret.at[e], send_sem=r_send, recv_sem=r_recv,
                    device_id=(to, t), device_id_type=MESH,
                ).start()
        if n == NC - 1:
            pltpu.make_async_remote_copy(
                src_ref=rows.at[31 - c], dst_ref=ret.at[e], send_sem=r_send, recv_sem=r_recv,
                device_id=(z * 2 + 1 - c, t), device_id_type=MESH,
            ).start()
            ret[e] = rows[30 + c]

    def collect():
        arriving[9].wait()
        bytes_of(ret.at[pl.ds(0, 31)], r_recv)
        back = ret[...].reshape(1024, 256)
        w0, w1 = column(rw_ref[0:1]), column(rw_ref[1:2])
        out_b[...] = (mm(sel0[...], back) * w0 + mm(sel1[...], back) * w1).astype(BF)
        pltpu.make_async_copy(out_b, far_b, out_sem.at[1]).start()

    stages = [
        arrive, relay, project, partial_sum, activate,
        lambda n: hid_steps[n][1](), lambda n: hid_steps[n][2](), lambda n: hid_steps[n][3](), finish,
        lambda n: pass_weights(), near_weights, lambda n: scan_prior(), lambda n: cell_out(),
        lambda n: mix_relay(), lambda n: mix_part(), lambda n: mix_sum(), lambda n: mix_out(),
        dispatch, lambda n: far_weights(), lambda n: weights_out(), lambda n: states(),
    ]
    for which, n in ORDER:
        stages[which](n)
    collect()

    bytes_of(wt.at[pl.ds(0, 3)], w_send)
    bytes_of(wr, far_send)
    bytes_of(wm.at[pl.ds(0, 3)], mw_send)
    bytes_of(hid.at[:, 0, pl.ds(0, 3)], ag_near)
    bytes_of(hid.at[:, pl.ds(0, 3)], ag_wide)
    bytes_of(mixed.at[pl.ds(0, 3)], ma_send)
    bytes_of(mfar, mr_send.at[0])
    bytes_of(msend, mr_send.at[1])
    bytes_of(xa.at[:, pl.ds(0, 3)], xg_send)
    bytes_of(gfar, g_send.at[0])
    bytes_of(gsend, g_send.at[1])
    bytes_of(p1s.at[pl.ds(0, 31)], p_send.at[0])
    bytes_of(p2s.at[pl.ds(0, 31)], p_send.at[1])
    bytes_of(xs.at[pl.ds(0, 31)], d_send)
    bytes_of(rows.at[pl.ds(0, 31)], r_send)
    pltpu.make_async_copy(out_a, far_a, out_sem.at[0]).wait()
    pltpu.make_async_copy(out_b, far_b, out_sem.at[1]).wait()


def pass_on(a_in, b_in, a_out, b_out, a_mid, b_mid, sem):
    ins = [pltpu.make_async_copy(a_in, a_mid, sem.at[0]), pltpu.make_async_copy(b_in, b_mid, sem.at[1])]
    outs = [pltpu.make_async_copy(a_mid, a_out, sem.at[2]), pltpu.make_async_copy(b_mid, b_out, sem.at[3])]
    for copy in ins:
        copy.start()
    for copy, onward in zip(ins, outs):
        copy.wait()
        onward.start()
    for copy in outs:
        copy.wait()


def body(q, k, v, ig, fg, og, gain, mixw, xin, routes, rw, gate, up, down):
    hbm = pl.BlockSpec(memory_space=pl.ANY)
    dma = pltpu.SemaphoreType.DMA
    out_a, out_b = pl.pallas_call(
        kernel,
        out_shape=(jax.ShapeDtypeStruct((512, 256), BF), jax.ShapeDtypeStruct((256, 256), BF)),
        in_specs=[hbm] * 14,
        out_specs=(hbm, hbm),
        scratch_shapes=[
            pltpu.VMEM((512, 128), BF),
            pltpu.VMEM((512, 128), BF),
            pltpu.VMEM((512, 256), BF),
            pltpu.VMEM((1, 512), F32),
            pltpu.VMEM((1, 512), F32),
            pltpu.VMEM((512, 256), BF),
            pltpu.VMEM((1, 256), F32),
            pltpu.VMEM((256, 256), BF),
            pltpu.VMEM((2, 256), jnp.int32),
            pltpu.VMEM((2, 256), F32),
            pltpu.VMEM((512, 256), BF),
            pltpu.VMEM((256, 256), BF),
            pltpu.VMEM((4, 4, 256, 256), BF),
            pltpu.VMEM((2, 2, 256, 256), BF),
            pltpu.VMEM((1024, 256), BF),
            pltpu.VMEM((1024, 256), BF),
            pltpu.VMEM((4, 128, 1024), BF),
            pltpu.VMEM((32, 32, 256), BF),
            pltpu.VMEM((NC, 4, S, 256), BF),
            pltpu.VMEM((NC, 2, 144, S), BF),
            pltpu.VMEM((NC, 2, 144, S), BF),
            pltpu.VMEM((NC, 144, S), BF),
            pltpu.VMEM((NC, 144, S), BF),
            pltpu.VMEM((NC, 4, 128, S), F32),
            pltpu.VMEM((NC, 16, S), F32),
            pltpu.VMEM((NC, 4, 4, 64, S), BF),
            pltpu.VMEM((32, 32, 256), BF),
            pltpu.VMEM((32, 32, 256), BF),
            pltpu.VMEM((4, 512, 256), BF),
            pltpu.VMEM((2, 256, 256), BF),
            pltpu.VMEM((2, 256, 256), BF),
            pltpu.VMEM((2, 512, 256), BF),
            pltpu.VMEM((2, 512, 256), BF),
            pltpu.VMEM((4, 512, 256), F32),
            pltpu.VMEM((32, 16, 128), BF),
            pltpu.VMEM((32, 16, 128), BF),
            pltpu.VMEM((32, 8, 128), BF),
            pltpu.VMEM((32, 8, 128), BF),
            pltpu.VMEM((32, 8, 128), F32),
            pltpu.VMEM((256, 1024), BF),
            pltpu.VMEM((256, 1024), BF),
            pltpu.VMEM((512, 256), F32),
            pltpu.VMEM((512, 128), F32),
            dma((10,)),
            dma((2,)),
            dma((3,)),
            dma,
            dma,
            dma,
            dma((2,)),
            dma((2,)),
            dma,
            dma((NC,)),
            dma,
            dma((NC, 2)),
            dma,
            dma,
            dma,
            dma,
            dma,
            dma((2,)),
            dma((2,)),
            dma((2,)),
            dma((2,)),
            dma((NC, 2)),
            dma,
            dma,
            dma((NC, 4)),
            dma,
            dma,
        ],
        compiler_params=pltpu.CompilerParams(
            collective_id=0, has_side_effects=True, vmem_limit_bytes=56 * 1024 * 1024
        ),
    )(q, k, v, ig, fg, og, gain.reshape(1, 256), mixw.reshape(4, 4, 256, 256), xin, routes.T, rw.T, gate[0], up[0], down[0])
    return pl.pallas_call(
        pass_on,
        out_shape=(jax.ShapeDtypeStruct((512, 256), BF), jax.ShapeDtypeStruct((256, 256), BF)),
        in_specs=[hbm] * 2,
        out_specs=(hbm, hbm),
        scratch_shapes=[pltpu.VMEM((512, 256), BF), pltpu.VMEM((256, 256), BF), dma((4,))],
    )(out_a, out_b)


def solution(mesh):
    in_specs = (
        P("ep", "tp"), P("ep", "tp"), P("ep", "tp"), P("tp", "ep"), P("tp", "ep"), P("ep", "tp"), P("tp"),
        P(None, "tp"), P("ep", "tp"), P("ep", None), P("ep", None), P("ep", "tp", None), P("ep", "tp", None),
        P("ep", None, "tp"),
    )
    return jax.shard_map(
        body, mesh=mesh, in_specs=in_specs, out_specs=(P("ep", "tp"), P("ep", "tp")), check_vma=False
    )
```

```python
import functools

import jax
import jax.numpy as jnp
from jax import lax
from jax.experimental import pallas as pl
from jax.experimental.pallas import tpu as pltpu
from jax.sharding import PartitionSpec as P

MESH = pl.DeviceIdType.MESH
BF, F32 = jnp.bfloat16, jnp.float32
D = 4096
EPS = 1e-6
FLOOR = -1e30
NEG = -3e38
SCALE = 128**-0.5
NC = 8
PER = 16 // NC
S = 1024 // NC
HOPS = [7, 9, 6, 10, 5, 11, 4, 12, 3, 13, 2, 14, 1, 15, 8, 0]
X_FIRST = [0, 1, 1, 0, 0, 0, 0, 0]
ORDER = [
    (10, 1), (17, 7), (10, 2), (17, 1), (19, 0), (21, 0), (17, 0), (17, 6), (17, 4), (18, 0), (10, 0), (0, 1),
    (17, 3), (17, 5), (0, 7), (0, 6), (1, 1), (17, 2), (0, 0), (1, 7), (0, 4), (20, 0), (2, 1), (1, 0),
    (0, 3), (2, 7), (1, 4), (0, 5), (3, 1), (2, 0), (3, 7), (1, 3), (4, 1), (0, 2), (2, 4), (3, 0),
    (1, 6), (5, 1), (4, 7), (1, 5), (2, 3), (3, 4), (1, 2), (9, 0), (4, 0), (11, 0), (6, 1), (2, 6),
    (2, 5), (5, 0), (4, 4), (5, 7), (3, 3), (2, 2), (7, 1), (3, 5), (6, 0), (3, 6), (5, 4), (4, 3),
    (6, 7), (8, 1), (3, 2), (7, 0), (4, 6), (6, 4), (4, 5), (5, 3), (12, 0), (4, 2), (7, 7), (8, 0),
    (5, 6), (6, 3), (5, 2), (7, 4), (5, 5), (8, 7), (10, 3), (7, 3), (13, 0), (6, 2), (8, 4), (6, 6),
    (6, 5), (13, 1), (22, 0), (14, 0), (7, 2), (8, 3), (7, 6), (7, 5), (14, 1), (8, 2), (15, 0), (8, 5),
    (15, 1), (8, 6), (16, 0), (16, 1),
]
NT = (((1,), (1,)), ((), ()))
TN = (((0,), (0,)), ((), ()))


def mm(a, b):
    return jnp.dot(a, b, preferred_element_type=F32)


def dg(a, b, dims):
    return lax.dot_general(a, b, dims, preferred_element_type=F32)


def kernel(
    q_hbm, k_hbm, v_hbm, ig_hbm, fg_hbm, og_hbm, gain_hbm, mixw_hbm, x_hbm, routes_hbm, rw_hbm,
    gate_hbm, up_hbm, down_hbm,
    far_a, far_b,
    q_ref, k_ref, v_ref, ig_ref, fg_ref, og_ref, gain_ref, x_ref, routes_ref, rw_ref, out_a, out_b,
    dwait, rwait, wm, wr, downn, downt, wt, xs, xa, gsend, grecv, gfar, ggot, gown, qown, hid, rows, ret, mixed, mfar, mgot, msend, mrecv, mown,
    p1s, p1r, p2s, p2r, seen, sel0, sel1, num_ref, col_ref,
    in_sem, out_sem, loc_sem, own_sem, w_send, w_recv, p_send, p_recv, d_send, d_recv,
    xg_send, xg_recv, far_send, far_recv, mw_send, mw_recv, ma_send, ma_recv, mr_send, mr_recv, g_send, g_recv,
    ag_near, ag_wide, ag_recv, r_send, r_recv, t_send, t_recv,
):
    e, t = lax.axis_index("ep"), lax.axis_index("tp")
    z, c = e // 2, e % 2
    y, x = t // 4, t % 4

    def along(axis, d):
        return (e, y * 4 + (x + d) % 4) if axis == "x" else (e, ((y + d) % 4) * 4 + x)

    def send(src, dst, ss, rs, dev):
        copy = pltpu.make_async_remote_copy(
            src_ref=src, dst_ref=dst, send_sem=ss, recv_sem=rs, device_id=dev, device_id_type=MESH
        )
        copy.start()

    def bytes_of(ref, sem):
        pltpu.make_async_copy(ref, ref, sem).wait()

    live = {}

    def once(name):
        fresh = name not in live
        live[name] = True
        return fresh

    barrier = pltpu.get_barrier_semaphore()

    def hello(k, _):
        pl.semaphore_signal(barrier, inc=1, device_id=((e + k) % 32, t), device_id_type=MESH)
        return 0

    lax.fori_loop(1, 32, hello, 0)
    for axis in "xy":
        for d in (1, 2, 3):
            pl.semaphore_signal(barrier, inc=1, device_id=along(axis, d), device_id_type=MESH)

    arriving = []
    for j, (src, dst) in enumerate((
        (routes_hbm, routes_ref), (x_hbm, x_ref), (fg_hbm, fg_ref), (ig_hbm, ig_ref), (k_hbm, k_ref), (v_hbm, v_ref),
        (q_hbm, q_ref), (og_hbm, og_ref), (gain_hbm, gain_ref), (rw_hbm, rw_ref),
    )):
        copy = pltpu.make_async_copy(src, dst, in_sem.at[j])
        copy.start()
        arriving.append(copy)

    own_g = pltpu.make_async_copy(
        gate_hbm.at[:, pl.ds(pl.multiple_of(y * 1024, 1024), 1024)], wt.at[y, pl.ds(0, 64)], own_sem
    )
    own_u = pltpu.make_async_copy(
        up_hbm.at[:, pl.ds(pl.multiple_of(y * 1024, 1024), 1024)], wt.at[y, pl.ds(64, 64)], own_sem
    )
    own_g.start()
    own_u.start()
    load_mix = pltpu.make_async_copy(mixw_hbm.at[:, x], wm.at[x], loc_sem.at[0])
    load_down = pltpu.make_async_copy(down_hbm, downn, loc_sem.at[1])
    load_mix.start()
    load_down.start()
    turned = []
    for b in range(16 if not all(X_FIRST) else 0):
        copy = pltpu.make_async_copy(
            down_hbm.at[pl.ds(64 * ((b % 4) * 4 + b // 4), 64)], downt.at[pl.ds(64 * b, 64)], loc_sem.at[2]
        )
        copy.start()
        turned.append(copy)


    arriving[0].wait()
    ei = lax.broadcasted_iota(jnp.int32, (256, 128), 1)
    di = lax.broadcasted_iota(jnp.int32, (256, 256), 0) == lax.broadcasted_iota(jnp.int32, (256, 256), 1)

    def column(row):
        return jnp.sum(jnp.where(di, row, 0.0), axis=1, keepdims=True)

    r0, r1 = (column(routes_ref[j : j + 1].astype(F32)) for j in (0, 1))
    ei = ei.astype(F32)
    hot0, hot1 = (ei == r0).astype(F32), (ei == r1).astype(F32)
    low = (
        lax.broadcasted_iota(jnp.int32, (256, 256), 1) < lax.broadcasted_iota(jnp.int32, (256, 256), 0)
    ).astype(F32).astype(BF)
    cum0 = mm(low, hot0.astype(BF))
    cum1 = mm(low, hot1.astype(BF)) + jnp.sum(hot0, axis=0, keepdims=True)
    s0 = r0 * 32.0 + jnp.sum(hot0 * cum0, axis=1, keepdims=True)
    s1 = r1 * 32.0 + jnp.sum(hot1 * cum1, axis=1, keepdims=True)
    arriving[1].wait()
    slot = lax.broadcasted_iota(jnp.int32, (256, 1024), 1).astype(F32)
    sel0[...] = (slot == s0).astype(F32).astype(BF)
    sel1[...] = (slot == s1).astype(F32).astype(BF)
    for b in range(4):
        lanes = slice(256 * b, 256 * b + 256)
        both = sel0[:, lanes] + sel1[:, lanes]
        xs[8 * b : 8 * b + 8] = dg(both, x_ref[...], TN).astype(BF).reshape(8, 32, 256)
    own_rows = pl.ds(pl.multiple_of(S - 64 + 32 * c, 32), 32)
    xa[NC - 1, x, own_rows, :] = xs[e]

    def dispatch(n):
        for i in range(PER * n, PER * n + PER):
            at = pl.ds(pl.multiple_of(64 * (i - PER * n) + 32 * c, 32), 32)
            for other in (1, 0) if i < 15 else (1,):
                to = ((z - HOPS[i] + 16) % 16) * 2 + (c + other) % 2
                if HOPS[i] == 8:
                    to = ((z + 8) % 16) * 2 + 1 - other
                if HOPS[i] == 8 and other == 0:
                    pltpu.make_async_remote_copy(
                        src_ref=xs.at[to], dst_ref=dwait, send_sem=d_send, recv_sem=t_recv.at[0],
                        device_id=(((z + 15) % 16) * 2 + c, t), device_id_type=MESH,
                    ).start()
                    continue
                pltpu.make_async_remote_copy(
                    src_ref=xs.at[to], dst_ref=xa.at[n, x, at], send_sem=d_send, recv_sem=d_recv.at[n],
                    device_id=(to, t), device_id_type=MESH,
                ).start()

    pl.semaphore_wait(barrier, 37)
    def weights_out():
        for d in (1, 2, 3):
            cols = pl.ds(pl.multiple_of((y + d) % 4 * 1024, 1024), 1024)
            for src, half in ((gate_hbm, 0), (up_hbm, 64)):
                send(src.at[:, cols], wt.at[y, pl.ds(half, 64)], w_send, w_recv, along("y", d))

    def far_weights():
        for j, d in enumerate((1, 3)):
            send(mixw_hbm.at[pl.ds(2 * j, 2), (x + 2) % 4], wr.at[j], far_send, far_recv, along("x", d))

    si = lax.broadcasted_iota(jnp.int32, (128, 512), 1)
    ri = lax.broadcasted_iota(jnp.int32, (128, 512), 0)

    def states():
        for copy in arriving[2:6]:
            copy.wait()
        f = fg_ref[...]
        log_f = jnp.minimum(f, 0.0) - jnp.log1p(jnp.exp(-jnp.abs(f)))
        c_row = jnp.zeros((1, 512), F32)
        for b in range(4):
            ti = ri + 128 * b
            col_ref[128 * b : 128 * b + 128, 0:1] = jnp.sum(
                jnp.where(si <= ti, log_f, 0.0), axis=1, keepdims=True
            )
            f_col = jnp.sum(jnp.where(si == ti, log_f, 0.0), axis=1, keepdims=True)
            c_row = c_row + jnp.sum(jnp.where(ti <= si, f_col, 0.0), axis=0, keepdims=True)
        a_row = ig_ref[...] - c_row
        a_max = jnp.max(a_row, axis=1, keepdims=True)
        g_all = jnp.sum(log_f, axis=1, keepdims=True)
        mem = jnp.zeros((128, 256), F32)
        norm = jnp.zeros((1, 128), F32)
        for b in range(4):
            ti = ri + 128 * b
            col_ref[128 * b : 128 * b + 128, 1:2] = jnp.max(
                jnp.where(si <= ti, a_row, NEG), axis=1, keepdims=True
            )
            a_col = jnp.max(jnp.where(si == ti, a_row, NEG), axis=1, keepdims=True)
            kw = k_ref[128 * b : 128 * b + 128].astype(F32) * jnp.exp(a_col - a_max)
            norm = norm + jnp.sum(kw, axis=0, keepdims=True)
            mem = mem + dg(kw.astype(BF), v_ref[128 * b : 128 * b + 128], TN)
        lane = lax.broadcasted_iota(jnp.int32, (1, 128), 1)
        both = jnp.where(lane < 64, g_all, g_all + a_max)
        row = lax.broadcasted_iota(jnp.int32, (8, 128), 0)
        aux = jnp.zeros((8, 128), F32)
        for j, rest in enumerate((norm, both)):
            for n in range(3):
                part = rest.astype(BF).astype(F32)
                aux = jnp.where(row == 3 * j + n, part, aux)
                rest = rest - part
        for h in range(2):
            tiles = mem[:, 128 * h : 128 * h + 128].reshape(16, 8, 128)
            p1s[16 * h : 16 * h + 16] = jnp.concatenate(
                [tiles, jnp.broadcast_to(aux[None], (16, 8, 128))], axis=1
            ).astype(BF)
        p1r[e] = p1s[e]
        live["a_row"] = a_row

        def first(k, _):
            to = (e + k) % 32
            pltpu.make_async_remote_copy(
                src_ref=p1s.at[to], dst_ref=p1r.at[e], send_sem=p_send.at[0], recv_sem=p_recv.at[0],
                device_id=(to, t), device_id_type=MESH,
            ).start()
            return 0

        lax.fori_loop(1, 32, first, 0)

    def inside():
        a_row = live["a_row"]
        arriving[6].wait()
        for b in range(4):
            ti = ri + 128 * b
            w = 128 * b + 128
            at = slice(128 * b, w)
            s = dg(q_ref[at], k_ref[:w], NT) * SCALE
            gate = jnp.exp(jnp.where(si <= ti, a_row, NEG)[:, :w] - col_ref[at, 1:2])
            s = s * gate
            col_ref[at, 2:3] = jnp.sum(s, axis=1, keepdims=True)
            num_ref[at] = mm(s.astype(BF), v_ref[:w])

    def pass_weights():
        if "a_row" in live and once("inside"):
            inside()
        bytes_of(wr, far_recv)
        for j, d in enumerate((1, 3)):
            send(wr.at[j], wm.at[(x - d + 4) % 4, pl.ds(2 * j, 2)], mw_send, mw_recv, along("x", d))

    def near_weights(p):
        for d in (1, 3):
            send(mixw_hbm.at[p, (x + d) % 4], wm.at[x, p], mw_send, mw_recv, along("x", d))

    at8 = HOPS.index(8)

    def onward_rows():
        bytes_of(dwait, t_recv.at[0])
        at = pl.ds(pl.multiple_of(64 * (at8 % PER) + 32 * c, 32), 32)
        send(dwait, xa.at[at8 // PER, x, at], t_send, d_recv.at[at8 // PER], (((z + 9) % 16) * 2 + 1, t))

    def onward_results():
        bytes_of(rwait, t_recv.at[1])
        send(rwait, ret.at[(e + 2) % 32], t_send, r_recv, (((z + 9) % 16) * 2 + 1, t))

    def scan_prior():
        if once("inside"):
            inside()
        bytes_of(p1r.at[pl.ds(0, 31)], p_recv.at[0])

        m, n, cc = jnp.full((1, 128), FLOOR, F32), jnp.zeros((1, 128), F32), jnp.zeros((8, 128), F32)
        for k in range(32):
            p2s[k] = cc.astype(BF)
            seen[k, 0:1], seen[k, 1:2] = m, n
            if k < 31:
                got = p1r[k].astype(F32)
                n2 = got[8:9] + got[9:10] + got[10:11]
                both = got[11:12] + got[12:13] + got[13:14]
                g2, m2 = both[:, 0:1], both[:, 64:65]
                top = jnp.maximum(g2 + m, m2)
                k1, k2 = jnp.exp(g2 + m - top), jnp.exp(m2 - top)
                m, cc, n = top, k1 * cc + k2 * got[0:8], k1 * n + k2 * n2
        live["pm"], live["pn"] = seen[e, 0:1], seen[e, 1:2]
        p2r[e] = p2s[e]

        def second(k, _):
            to = (e + k) % 32
            pltpu.make_async_remote_copy(
                src_ref=p2s.at[to], dst_ref=p2r.at[e], send_sem=p_send.at[1], recv_sem=p_recv.at[1],
                device_id=(to, t), device_id_type=MESH,
            ).start()
            return 0

        lax.fori_loop(1, 32, second, 0)

    def gather_steps(buf, order, n, cut):
        inner, outer = order
        ci, co = (x, y) if inner == "x" else (y, x)
        near, wide, rs = ag_near, ag_wide, ag_recv

        def one():
            own = buf.at[co, ci]
            for d in (1, 3):
                send(own, own, near, rs.at[n, 0], along(inner, d))

        def two():
            bytes_of(buf.at[co, pl.ds(0, 2)], rs.at[n, 0])
            for j, d in enumerate((1, 3)):
                part = buf.at[co, (ci - d + 4) % 4, pl.ds(j * cut, cut)]
                send(part, part, near, rs.at[n, 1], along(inner, d))

        def three():
            bytes_of(buf.at[co, 0], rs.at[n, 1])
            own = buf.at[co]
            for d in (1, 3):
                send(own, own, wide, rs.at[n, 2], along(outer, d))

        def four():
            bytes_of(buf.at[pl.ds(0, 2)], rs.at[n, 2])
            for j, d in enumerate((1, 3)):
                part = buf.at[(co - d + 4) % 4, pl.ds(2 * j, 2)]
                send(part, part, wide, rs.at[n, 3], along(outer, d))

        def last():
            bytes_of(buf.at[0], rs.at[n, 3])

        return one, two, three, four, last

    hid_steps = [gather_steps(hid.at[n], "xy" if X_FIRST[n] else "yx", n, 32) for n in range(NC)]

    def cell_out():
        for copy in arriving[7:9]:
            copy.wait()
        bytes_of(p2r.at[pl.ds(0, 31)], p_recv.at[1])
        pm, pn = live["pm"][:, 0:1], live["pn"]
        parts = []
        for h in range(2):
            parts.append(p2r[16 * h : 16 * h + 16].reshape(128, 128))
        for b in range(4):
            at = slice(128 * b, 128 * b + 128)
            qb = q_ref[at]
            c_col, amx, den = col_ref[at, 0:1], col_ref[at, 1:2], col_ref[at, 2:3]
            local, inter = c_col + amx, c_col + pm
            top = jnp.maximum(local, inter)
            f_local, f_inter = jnp.exp(local - top), jnp.exp(inter - top) * SCALE
            qc = jnp.concatenate([mm(qb, part) for part in parts], axis=1)
            num = f_inter * qc + f_local * num_ref[at]
            den = f_inter * jnp.sum(qb.astype(F32) * pn, axis=1, keepdims=True) + f_local * den
            hv = num / jnp.maximum(jnp.abs(den), jnp.exp(-top))
            hv = hv * lax.rsqrt(jnp.mean(hv * hv, axis=1, keepdims=True) + EPS)
            hv = hv * gain_ref[...] * jax.nn.sigmoid(og_ref[at].astype(F32))
            h = b // 2
            mixed[h, y, 128 * (b % 2) : 128 * (b % 2) + 128, :] = hv.astype(BF)
            if b % 2:
                own = mixed.at[h, y]
                for d in (1, 3):
                    send(own, own, ma_send, ma_recv.at[h, 0], along("y", d))

    def mix_relay(h):
        bytes_of(mixed.at[h, pl.ds(0, 2)], ma_recv.at[h, 0])
        for j, d in enumerate((1, 3)):
            part = mixed.at[h, (y - d + 4) % 4, pl.ds(128 * j, 128)]
            send(part, part, ma_send, ma_recv.at[h, 1], along("y", d))

    def mix_part(h):
        bytes_of(mixed.at[h, 0], ma_recv.at[h, 1])
        if once("wm"):
            load_mix.wait()
            bytes_of(wm.at[pl.ds(0, 3)], mw_recv)
        for d in (2, 1, 3, 0):
            there = (x + d) % 4
            acc = mm(mixed[h, 0], wm[there, 0])
            for j in range(1, 4):
                acc = acc + mm(mixed[h, j], wm[there, j])
            if d == 2:
                mfar[h] = acc.astype(BF).reshape(2, 128, 256)
                for j, w in enumerate((1, 3)):
                    send(mfar.at[h, j], mgot.at[h, j], mr_send.at[0], mr_recv.at[h, 0], along("x", w))
            else:
                mown[h, d] = acc

    def mix_sum(h):
        bytes_of(mgot.at[h], mr_recv.at[h, 0])
        for j, d in enumerate((1, 3)):
            half = slice(128 * j, 128 * j + 128)
            rest = slice(128 - 128 * j, 256 - 128 * j)
            msend[h, j, half] = (mown[h, d, half] + mgot[h, j].astype(F32)).astype(BF)
            msend[h, j, rest] = mown[h, d, rest].astype(BF)
            send(msend.at[h, j], mrecv.at[h, j], mr_send.at[1], mr_recv.at[h, 1], along("x", d))

    def mix_out(h):
        bytes_of(mrecv.at[h], mr_recv.at[h, 1])
        at = pl.ds(256 * h, 256)
        out_a[256 * h : 256 * h + 256] = (mown[h, 0] + mrecv[h, 0].astype(F32) + mrecv[h, 1].astype(F32)).astype(BF)
        pltpu.make_async_copy(out_a.at[at], far_a.at[at], out_sem.at[0]).start()

    def arrive(n):
        k = 2 * PER if n < NC - 1 else 2 * PER - 1
        landed = xa.at[n, x, pl.ds(0, 32 * k)]
        bytes_of(landed, d_recv.at[n])
        own = xa.at[n, x]
        for d in (1, 3):
            send(own, own, xg_send, xg_recv.at[n, 0], along("x", d))

    def relay(n):
        bytes_of(xa.at[n, pl.ds(0, 2)], xg_recv.at[n, 0])
        for j, d in enumerate((1, 3)):
            part = xa.at[n, (x - d + 4) % 4, pl.ds(S // 2 * j, S // 2)]
            send(part, part, xg_send, xg_recv.at[n, 1], along("x", d))

    def project(n):
        bytes_of(xa.at[n, 0], xg_recv.at[n, 1])
        if once("wt"):
            bytes_of(wt.at[y], own_sem)
            bytes_of(wt.at[pl.ds(0, 3)], w_recv)
        acc = jnp.zeros((512, S), F32)
        sq = jnp.zeros((16, S), F32)
        ones = jnp.ones((16, 256), BF)
        for j in range(4):
            xx = xa[n, j]
            w = wt[:, :, 256 * j : 256 * j + 256].reshape(512, 256)
            acc = acc + dg(w, xx, NT)
            wide = xx.astype(F32)
            wide = wide * wide
            hi = wide.astype(BF)
            lo = (wide - hi.astype(F32)).astype(BF)
            sq = sq + dg(ones, hi, NT) + dg(ones, lo, NT)
        gown[n] = acc.reshape(4, 128, S)
        qown[n] = sq
        gfar[n, 0:128] = gown[n, (y + 2) % 4].astype(BF)
        gfar[n, 128:144] = in_three(sq)
        for j, d in enumerate((1, 3)):
            at = pl.ds(64 * j, 64 + 16 * j)
            send(gfar.at[n, at], ggot.at[n, at], g_send.at[0], g_recv.at[n, 0], along("y", d))

    def in_three(sq):
        hi = sq.astype(BF).astype(F32)
        mid = (sq - hi).astype(BF).astype(F32)
        row = lax.broadcasted_iota(jnp.int32, (16, S), 0)
        parts = jnp.where(row == 0, hi, jnp.where(row == 1, mid, jnp.where(row == 2, sq - hi - mid, 0.0)))
        return parts.astype(BF)

    def partial_sum(n):
        bytes_of(ggot.at[n], g_recv.at[n, 0])
        sq = qown[n]
        gsend[n, 0, 0:64] = (gown[n, (y + 1) % 4, 0:64] + ggot[n, 0:64].astype(F32)).astype(BF)
        gsend[n, 0, 64:128] = gown[n, (y + 1) % 4, 64:128].astype(BF)
        gsend[n, 0, 128:144] = in_three(sq)
        gsend[n, 1, 0:64] = gown[n, (y + 3) % 4, 0:64].astype(BF)
        gsend[n, 1, 64:128] = (gown[n, (y + 3) % 4, 64:128] + ggot[n, 64:128].astype(F32)).astype(BF)
        gsend[n, 1, 128:144] = in_three(sq + jnp.sum(ggot[n, 128:144].astype(F32), axis=0, keepdims=True))
        for j, d in enumerate((1, 3)):
            send(gsend.at[n, j], grecv.at[n, j], g_send.at[1], g_recv.at[n, 1], along("y", d))

    def activate(n):
        bytes_of(grecv.at[n], g_recv.at[n, 1])
        total = gown[n, y] + grecv[n, 0, 0:128].astype(F32) + grecv[n, 1, 0:128].astype(F32)
        sq = qown[n, 0:1] + jnp.sum(
            grecv[n, 0, 128:144].astype(F32) + grecv[n, 1, 128:144].astype(F32), axis=0, keepdims=True
        )
        inv = lax.rsqrt(sq / D + EPS)
        g, u = total[0:64] * inv, total[64:128] * inv
        o, i = (y, x) if X_FIRST[n] else (x, y)
        hid[n, o, i] = (g * jax.nn.sigmoid(g) * u).astype(BF)
        hid_steps[n][0]()

    def finish(n):
        hid_steps[n][4]()
        if once("down"):
            load_down.wait()
            if turned:
                bytes_of(downt, loc_sem.at[2])
        down = downn if X_FIRST[n] else downt
        res = dg(hid[n].reshape(1024, S), down[...], TN).astype(BF)
        rows[2 * PER * n : 2 * PER * n + 2 * PER] = res.reshape(2 * PER, 32, 256)
        for b in range(2 * PER):
            i, cs = PER * n + b // 2, b % 2
            if i < 15:
                to = ((z + HOPS[i]) % 16) * 2 + cs
                if HOPS[i] == 8 and cs == 1:
                    pltpu.make_async_remote_copy(
                        src_ref=rows.at[2 * PER * n + b], dst_ref=rwait, send_sem=r_send, recv_sem=t_recv.at[1],
                        device_id=(((z + 15) % 16) * 2 + c, t), device_id_type=MESH,
                    ).start()
                    continue
                pltpu.make_async_remote_copy(
                    src_ref=rows.at[2 * PER * n + b], dst_ref=ret.at[e], send_sem=r_send, recv_sem=r_recv,
                    device_id=(to, t), device_id_type=MESH,
                ).start()
        if n == NC - 1:
            pltpu.make_async_remote_copy(
                src_ref=rows.at[31 - c], dst_ref=ret.at[e], send_sem=r_send, recv_sem=r_recv,
                device_id=(z * 2 + 1 - c, t), device_id_type=MESH,
            ).start()
            ret[e] = rows[30 + c]

    def collect():
        arriving[9].wait()
        bytes_of(ret.at[pl.ds(0, 31)], r_recv)
        back = ret[...].reshape(1024, 256)
        w0, w1 = column(rw_ref[0:1]), column(rw_ref[1:2])
        out_b[...] = (mm(sel0[...], back) * w0 + mm(sel1[...], back) * w1).astype(BF)
        pltpu.make_async_copy(out_b, far_b, out_sem.at[1]).start()

    stages = [
        arrive, relay, project, partial_sum, activate,
        lambda n: hid_steps[n][1](), lambda n: hid_steps[n][2](), lambda n: hid_steps[n][3](), finish,
        lambda n: pass_weights(), near_weights, lambda n: scan_prior(), lambda n: cell_out(),
        mix_relay, mix_part, mix_sum, mix_out,
        dispatch, lambda n: far_weights(), lambda n: weights_out(), lambda n: states(),
        lambda n: onward_rows(), lambda n: onward_results(),
    ]
    for which, n in ORDER:
        stages[which](n)
    collect()

    bytes_of(wt.at[pl.ds(0, 3)], w_send)
    bytes_of(wr, far_send)
    bytes_of(xs.at[pl.ds(0, 2)], t_send)
    bytes_of(wm.at[pl.ds(0, 3)], mw_send)
    bytes_of(hid.at[:, 0, pl.ds(0, 3)], ag_near)
    bytes_of(hid.at[:, pl.ds(0, 3)], ag_wide)
    bytes_of(mixed.at[:, pl.ds(0, 3)], ma_send)
    bytes_of(mfar, mr_send.at[0])
    bytes_of(msend, mr_send.at[1])
    bytes_of(xa.at[:, pl.ds(0, 3)], xg_send)
    bytes_of(gfar, g_send.at[0])
    bytes_of(gsend, g_send.at[1])
    bytes_of(p1s.at[pl.ds(0, 31)], p_send.at[0])
    bytes_of(p2s.at[pl.ds(0, 31)], p_send.at[1])
    bytes_of(xs.at[pl.ds(0, 31)], d_send)
    bytes_of(rows.at[pl.ds(0, 31)], r_send)
    pltpu.make_async_copy(out_a, far_a, out_sem.at[0]).wait()
    pltpu.make_async_copy(out_b, far_b, out_sem.at[1]).wait()


def pass_on(a_in, b_in, a_out, b_out, a_mid, b_mid, sem):
    ins = [pltpu.make_async_copy(a_in, a_mid, sem.at[0]), pltpu.make_async_copy(b_in, b_mid, sem.at[1])]
    outs = [pltpu.make_async_copy(a_mid, a_out, sem.at[2]), pltpu.make_async_copy(b_mid, b_out, sem.at[3])]
    for copy in ins:
        copy.start()
    for copy, onward in zip(ins, outs):
        copy.wait()
        onward.start()
    for copy in outs:
        copy.wait()


def body(q, k, v, ig, fg, og, gain, mixw, xin, routes, rw, gate, up, down):
    hbm = pl.BlockSpec(memory_space=pl.ANY)
    dma = pltpu.SemaphoreType.DMA
    out_a, out_b = pl.pallas_call(
        kernel,
        out_shape=(jax.ShapeDtypeStruct((512, 256), BF), jax.ShapeDtypeStruct((256, 256), BF)),
        in_specs=[hbm] * 14,
        out_specs=(hbm, hbm),
        scratch_shapes=[
            pltpu.VMEM((512, 128), BF),
            pltpu.VMEM((512, 128), BF),
            pltpu.VMEM((512, 256), BF),
            pltpu.VMEM((1, 512), F32),
            pltpu.VMEM((1, 512), F32),
            pltpu.VMEM((512, 256), BF),
            pltpu.VMEM((1, 256), F32),
            pltpu.VMEM((256, 256), BF),
            pltpu.VMEM((2, 256), jnp.int32),
            pltpu.VMEM((2, 256), F32),
            pltpu.VMEM((512, 256), BF),
            pltpu.VMEM((256, 256), BF),
            pltpu.VMEM((32, 256), BF),
            pltpu.VMEM((32, 256), BF),
            pltpu.VMEM((4, 4, 256, 256), BF),
            pltpu.VMEM((2, 2, 256, 256), BF),
            pltpu.VMEM((1024, 256), BF),
            pltpu.VMEM((1024, 256), BF),
            pltpu.VMEM((4, 128, 1024), BF),
            pltpu.VMEM((32, 32, 256), BF),
            pltpu.VMEM((NC, 4, S, 256), BF),
            pltpu.VMEM((NC, 2, 144, S), BF),
            pltpu.VMEM((NC, 2, 144, S), BF),
            pltpu.VMEM((NC, 144, S), BF),
            pltpu.VMEM((NC, 144, S), BF),
            pltpu.VMEM((NC, 4, 128, S), F32),
            pltpu.VMEM((NC, 16, S), F32),
            pltpu.VMEM((NC, 4, 4, 64, S), BF),
            pltpu.VMEM((32, 32, 256), BF),
            pltpu.VMEM((32, 32, 256), BF),
            pltpu.VMEM((2, 4, 256, 256), BF),
            pltpu.VMEM((2, 2, 128, 256), BF),
            pltpu.VMEM((2, 2, 128, 256), BF),
            pltpu.VMEM((2, 2, 256, 256), BF),
            pltpu.VMEM((2, 2, 256, 256), BF),
            pltpu.VMEM((2, 4, 256, 256), F32),
            pltpu.VMEM((32, 16, 128), BF),
            pltpu.VMEM((32, 16, 128), BF),
            pltpu.VMEM((32, 8, 128), BF),
            pltpu.VMEM((32, 8, 128), BF),
            pltpu.VMEM((32, 8, 128), F32),
            pltpu.VMEM((256, 1024), BF),
            pltpu.VMEM((256, 1024), BF),
            pltpu.VMEM((512, 256), F32),
            pltpu.VMEM((512, 128), F32),
            dma((10,)),
            dma((2,)),
            dma((3,)),
            dma,
            dma,
            dma,
            dma((2,)),
            dma((2,)),
            dma,
            dma((NC,)),
            dma,
            dma((NC, 2)),
            dma,
            dma,
            dma,
            dma,
            dma,
            dma((2, 2)),
            dma((2,)),
            dma((2, 2)),
            dma((2,)),
            dma((NC, 2)),
            dma,
            dma,
            dma((NC, 4)),
            dma,
            dma,
            dma,
            dma((2,)),
        ],
        compiler_params=pltpu.CompilerParams(
            collective_id=0, has_side_effects=True, vmem_limit_bytes=56 * 1024 * 1024
        ),
    )(q, k, v, ig, fg, og, gain.reshape(1, 256), mixw.reshape(4, 4, 256, 256), xin, routes.T, rw.T, gate[0], up[0], down[0])
    return pl.pallas_call(
        pass_on,
        out_shape=(jax.ShapeDtypeStruct((512, 256), BF), jax.ShapeDtypeStruct((256, 256), BF)),
        in_specs=[hbm] * 2,
        out_specs=(hbm, hbm),
        scratch_shapes=[pltpu.VMEM((512, 256), BF), pltpu.VMEM((256, 256), BF), dma((4,))],
    )(out_a, out_b)


def solution(mesh):
    in_specs = (
        P("ep", "tp"), P("ep", "tp"), P("ep", "tp"), P("tp", "ep"), P("tp", "ep"), P("ep", "tp"), P("tp"),
        P(None, "tp"), P("ep", "tp"), P("ep", None), P("ep", None), P("ep", "tp", None), P("ep", "tp", None),
        P("ep", None, "tp"),
    )
    return jax.shard_map(
        body, mesh=mesh, in_specs=in_specs, out_specs=(P("ep", "tp"), P("ep", "tp")), check_vma=False
    )
```
